512 devices in a mesh: sp: 128 (over z, x, core), tp: 4 (over y).
Axes of the slice: x: 4, y: 4, z: 16, core: 2. Of those that a mesh axis runs over, the one named last changes fastest.
Arguments:
- tokens: bfloat16 [16384, 2048], P('sp'), may hold values from -6 to 6
- pre_gain: float32 [2048], replicated, may hold values from 0.1 to 1.9
- outer_gate: bfloat16 [2048, 1024], P('sp', 'tp'), may hold values from -0.125 to 0.125
- inner_gate: bfloat16 [2048, 1024], P('sp', 'tp'), may hold values from -0.125 to 0.125
- conv_input: bfloat16 [2048, 1024], P('sp', 'tp'), may hold values from -0.125 to 0.125
- conv_taps: float32 [3, 1024], P(None, 'tp'), may hold values from -3.5 to 3.5
- query_down: bfloat16 [2048, 768], P(None, 'tp'), may hold values from -0.088388348 to 0.088388348
- latent_down: bfloat16 [2048, 512], P(None, 'tp'), may hold values from -0.088388348 to 0.088388348
- rotary_down: bfloat16 [2048, 32], replicated, may hold values from -0.125 to 0.125
- query_gain: float32 [768], replicated, may hold values from 1 to 3
- latent_gain: float32 [512], replicated, may hold values from 1 to 3
- query_up: bfloat16 [768, 512], P(None, 'tp'), may hold values from -0.14433757 to 0.14433757
- query_rotary: bfloat16 [768, 256], P(None, 'tp'), may hold values from -0.21875 to 0.21875
- key_up: bfloat16 [512, 512], P(None, 'tp'), may hold values from -4.33012702 to 4.33012702
- value_up: bfloat16 [512, 512], P(None, 'tp'), may hold values from -0.25 to 0.25
- conv_output: bfloat16 [1024, 2048], P('tp'), may hold values from -0.15625 to 0.15625
- heads_output: bfloat16 [512, 2048], P('tp'), may hold values from -0.15625 to 0.15625
- post_gain: float32 [2048], replicated, may hold values from 0.1 to 1.9
Outputs:
- mixed: bfloat16 [16384, 2048], P(('sp', 'tp'))
- row_logsum: float32 [8, 16384], P('tp', 'sp')
The draws below stay inside these ranges and needn't reach their ends.
All inputs are finite; a program needn't handle non-finite values.
Results may differ from the reference program's by a relative error of at most 0.013.
Values may be sent and summed in bfloat16 or wider, within the bound.
No kernel may reach another device: no remote copies, remote signals or barrier semaphores. Data moves between devices by JAX's collectives and lax.ppermute only.
A program may use at most 64 MiB of HBM per device.

```python
import math
import jax
import jax.numpy as jnp
from jax import lax

D = 2048
D_CONV = 1024
HEADS = 8
NOPE = 64
ROPE = 32
VDIM = 64
QLAT = 768
KVLAT = 512
TAPS = 3
TOKENS = 16384


def clipped(key, shape, fan_in):
    return jnp.clip(jax.random.normal(key, shape, jnp.float32), -3.95, 3.95) * fan_in ** (-0.5)


def shared_down(key):
    return clipped(jax.random.fold_in(key, 101), (D, QLAT), D)


def shared_up(key):
    return clipped(jax.random.fold_in(key, 103), (QLAT, HEADS * NOPE), QLAT)


def draw_query_down(key, part):
    return shared_down(key).astype(jnp.bfloat16)


def draw_latent_down(key, part):
    result = clipped(jax.random.fold_in(key, 102), (D, KVLAT), D)
    return result.astype(jnp.bfloat16)


def draw_query_up(key, part):
    return shared_up(key).astype(jnp.bfloat16)


def draw_key_up(key, part):
    result = clipped(jax.random.fold_in(key, 105), (KVLAT, HEADS * NOPE), KVLAT)
    return result.astype(jnp.bfloat16)


def block_levels(stream_key, shape, split, low, high):
    level = 1.0
    for dim, blocks in split:
        steps = jax.random.uniform(jax.random.fold_in(jax.random.fold_in(stream_key, 6), dim), (blocks,), jnp.float32, low / len(split), high / len(split))
        level = level * jnp.repeat(jnp.exp(steps), shape[dim] // blocks).reshape((-1,) + (1,) * (len(shape) - 1 - dim))
    return level


def gaussian(key, extent, spread, reach, shards=(), held_as=jnp.bfloat16):
    array = spread * jax.random.normal(key, extent, jnp.float32)
    if shards:
        array = array * block_levels(key, extent, shards, -0.22, 0.18)
    return jnp.clip(array, -reach, reach).astype(held_as)


def setup_inputs(seed: int = 0) -> dict:
    arg_keys = jax.random.split(jax.random.key(seed), 19)
    return {
        "tokens": gaussian(arg_keys[0], (TOKENS, D), 1.0, 6.0, ((0, 128),)),
        "pre_gain": jnp.clip(1.0 + 0.18 * jax.random.normal(arg_keys[1], (D,), jnp.float32), 0.1, 1.9),
        "outer_gate": gaussian(arg_keys[2], (D, D_CONV), D ** -0.5, 0.125, ((0, 128), (1, 4))),
        "inner_gate": gaussian(arg_keys[3], (D, D_CONV), D ** -0.5, 0.125, ((0, 128), (1, 4))),
        "conv_input": gaussian(arg_keys[4], (D, D_CONV), D ** -0.5, 0.125, ((0, 128), (1, 4))),
        "conv_taps": gaussian(arg_keys[5], (TAPS, D_CONV), TAPS ** -0.5, 3.5, ((1, 4),), jnp.float32),
        "query_down": draw_query_down(jax.random.fold_in(arg_keys[18], 71), 0),
        "latent_down": draw_latent_down(jax.random.fold_in(arg_keys[18], 71), 0),
        "rotary_down": gaussian(arg_keys[8], (D, ROPE), D ** -0.5, 0.125),
        "query_gain": jnp.clip(jnp.exp(jax.random.uniform(arg_keys[9], (QLAT,), jnp.float32, math.log(1.0), math.log(3.0))), 1.0, 3.0),
        "latent_gain": jnp.clip(jnp.exp(jax.random.uniform(arg_keys[10], (KVLAT,), jnp.float32, math.log(1.0), math.log(3.0))), 1.0, 3.0),
        "query_up": draw_query_up(jax.random.fold_in(arg_keys[18], 71), 0),
        "query_rotary": gaussian(arg_keys[12], (QLAT, HEADS * ROPE), QLAT ** -0.5, 0.21875, ((1, 4),)),
        "key_up": draw_key_up(jax.random.fold_in(arg_keys[18], 71), 0),
        "value_up": gaussian(arg_keys[14], (KVLAT, HEADS * VDIM), KVLAT ** -0.5, 0.25, ((1, 4),)),
        "conv_output": gaussian(arg_keys[15], (D_CONV, D), (D_CONV + HEADS * VDIM) ** -0.5, 0.15625, ((0, 4),)),
        "heads_output": gaussian(arg_keys[16], (HEADS * VDIM, D), (D_CONV + HEADS * VDIM) ** -0.5, 0.15625, ((0, 4),)),
        "post_gain": jnp.clip(1.0 + 0.18 * jax.random.normal(arg_keys[17], (D,), jnp.float32), 0.1, 1.9),
    }


eps = 1e-06
rope_theta = 500000.0

def rms_scale(values, scale_row):
    widened = values.astype(jnp.float32)
    return widened * lax.rsqrt(lax.optimization_barrier(jnp.mean(widened * widened, axis=-1, keepdims=True)) + eps) * scale_row

def rotate(values, positions):
    half_width = values.shape[-1] // 2
    frequency = rope_theta ** (-jnp.arange(half_width, dtype=jnp.float32) / half_width)
    angles = positions.astype(jnp.float32)[:, None] * frequency
    cosine = jnp.cos(angles)[:, None, :]
    sine_part = jnp.sin(angles)[:, None, :]
    leading = values[..., :half_width]
    trailing = values[..., half_width:]
    return jnp.concatenate([leading * cosine - trailing * sine_part, trailing * cosine + leading * sine_part], axis=-1)

def reference(tokens, pre_gain, outer_gate, inner_gate, conv_input, conv_taps, query_down, latent_down, rotary_down, query_gain, latent_gain, query_up, query_rotary, key_up, value_up, conv_output, heads_output, post_gain):
    normed = rms_scale(tokens, pre_gain).astype(jnp.bfloat16)
    positions = jnp.arange(TOKENS, dtype=jnp.int32)
    outer_part = jnp.dot(normed, outer_gate, preferred_element_type=jnp.float32)
    inner_part = jnp.dot(normed, inner_gate, preferred_element_type=jnp.float32)
    signal = jnp.dot(normed, conv_input, preferred_element_type=jnp.float32)
    product = (inner_part * signal).astype(jnp.bfloat16)
    extended = jnp.concatenate([jnp.zeros((TAPS - 1, D_CONV), jnp.float32), product.astype(jnp.float32)], axis=0)
    convolved = extended[0:TOKENS] * conv_taps[0]
    for offset in range(1, TAPS):
        convolved = convolved + extended[offset:offset + TOKENS] * conv_taps[offset]
    conv_mixed = (outer_part * convolved).astype(jnp.bfloat16)
    query_latent = jnp.dot(normed, query_down, preferred_element_type=jnp.float32).astype(jnp.bfloat16)
    key_latent = jnp.dot(normed, latent_down, preferred_element_type=jnp.float32).astype(jnp.bfloat16)
    query_normed = rms_scale(query_latent, query_gain).astype(jnp.bfloat16)
    latent_normed = rms_scale(key_latent, latent_gain).astype(jnp.bfloat16)
    rotary_raw = jnp.dot(normed, rotary_down, preferred_element_type=jnp.float32)
    key_rotary = rotate(rotary_raw[:, None, :], positions)[:, 0, :].astype(jnp.bfloat16)
    query_nope = jnp.dot(query_normed, query_up, preferred_element_type=jnp.float32).astype(jnp.bfloat16)
    query_nope = query_nope.reshape(TOKENS, HEADS, NOPE)
    turned_raw = jnp.dot(query_normed, query_rotary, preferred_element_type=jnp.float32)
    query_turned = rotate(turned_raw.reshape(TOKENS, HEADS, ROPE), positions).astype(jnp.bfloat16)
    key_nope = jnp.dot(latent_normed, key_up, preferred_element_type=jnp.float32).astype(jnp.bfloat16)
    key_nope = key_nope.reshape(TOKENS, HEADS, NOPE).astype(jnp.float32)
    value_rows = jnp.dot(latent_normed, value_up, preferred_element_type=jnp.float32).astype(jnp.bfloat16)
    value_rows = value_rows.reshape(TOKENS, HEADS, VDIM).astype(jnp.float32)
    key_wide = key_rotary.astype(jnp.float32)
    score_scale = (NOPE + ROPE) ** (-0.5)
    block_rows = 512 if TOKENS % 512 == 0 else TOKENS

    def one_block(block_index):
        first_row = block_index * block_rows
        query_block = lax.dynamic_slice_in_dim(query_nope, first_row, block_rows, 0).astype(jnp.float32)
        turned_block = lax.dynamic_slice_in_dim(query_turned, first_row, block_rows, 0).astype(jnp.float32)
        scores = jnp.einsum('qhd,khd->hqk', query_block, key_nope)
        scores = scores + jnp.einsum('qhd,kd->hqk', turned_block, key_wide)
        scores = scores * score_scale
        query_position = first_row + jnp.arange(block_rows, dtype=jnp.int32)
        causal = positions[None, :] <= query_position[:, None]
        scores = jnp.where(causal[None], scores, -1e+30)
        row_best = lax.optimization_barrier(jnp.max(scores, axis=-1))
        weights = jnp.where(causal[None], jnp.exp(scores - row_best[..., None]), 0.0)
        weight_sum = lax.optimization_barrier(jnp.sum(weights, axis=-1))
        rounded = lax.optimization_barrier(weights.astype(jnp.bfloat16))
        weighted = jnp.einsum('hqk,khd->hqd', rounded.astype(jnp.float32), value_rows)
        mixed_block = (weighted / weight_sum[..., None]).astype(jnp.bfloat16)
        return (mixed_block, row_best + jnp.log(weight_sum))
    blocks_out, logsums = lax.map(one_block, jnp.arange(TOKENS // block_rows, dtype=jnp.int32))
    heads_mixed = blocks_out.transpose(0, 2, 1, 3).reshape(TOKENS, HEADS * VDIM)
    row_logsum = logsums.transpose(1, 0, 2).reshape(HEADS, TOKENS)
    projected = jnp.dot(conv_mixed, conv_output, preferred_element_type=jnp.float32)
    projected = projected + jnp.dot(heads_mixed, heads_output, preferred_element_type=jnp.float32)
    mixed = rms_scale(projected, post_gain).astype(jnp.bfloat16)
    return (mixed, row_logsum)
```

```python
import functools
import math

import jax
import jax.numpy as jnp
from jax import lax
from jax.experimental import pallas as pl
from jax.experimental.pallas import tpu as pltpu
from jax.sharding import Mesh
from jax.sharding import PartitionSpec as P

NOPE = 64
ROPE = 32
VDIM = 64
TAPS = 3
SP = ("sp_0", "sp_1", "sp_2")
SP_TP = ("sp_0", "sp_1", "sp_2", "tp")
GROUP = ("sp_1", "sp_2")

eps = 1e-06
rope_theta = 500000.0
SCALE = (NOPE + ROPE) ** (-0.5)
LOG2E = math.log2(math.e)
LOW = -1e30
BF16 = jnp.bfloat16
F32 = jnp.float32


def copy_for_each(array, axis):
    copies = jnp.broadcast_to(array, (lax.axis_size(axis), *array.shape))
    return lax.all_to_all(copies, axis, split_axis=0, concat_axis=0, tiled=True)


def exchange(array, axis):
    return lax.all_to_all(array, axis, split_axis=0, concat_axis=0, tiled=True)


def shifted(value, axis, steps):
    count = lax.axis_size(axis)
    first, last = (max(0, -steps), min(count, count - steps))
    return lax.ppermute(value, axis, [(source, source + steps) for source in range(first, last)])


def rms_scale(values, scale_row):
    widened = values.astype(F32)
    return (
        widened * lax.rsqrt(jnp.mean(widened * widened, axis=-1, keepdims=True) + eps) * scale_row
    )


def dot_t(values, weights):
    return lax.dot_general(weights, values, (((0,), (1,)), ((), ())), preferred_element_type=F32)


def rotate_rows(values, cosine, sine):
    half = values.shape[-2] // 2
    leading = values[..., :half, :]
    trailing = values[..., half:, :]
    return jnp.concatenate(
        [leading * cosine - trailing * sine, trailing * cosine + leading * sine], axis=-2
    )


KEYS = 256
COLS = 512


def attention_kernel(
    place, key_ref, value_ref, query_ref, out_ref, key_rows, value_cols, query_full, best, total, acc
):
    z = place[0]
    j = place[1]
    blocks = key_ref.shape[0]
    groups = query_ref.shape[0]
    queries = groups * 128
    width = 2 * queries
    for b in range(blocks):
        key_rows[b * 128 : (b + 1) * 128, :] = key_ref[b].T
        value_cols[:, b * 128 : (b + 1) * 128] = value_ref[b]
    for h in range(2):
        for g in range(groups):
            at = slice(h * queries + g * 128, h * queries + (g + 1) * 128)
            query_full[h * 64 : (h + 1) * 64, at] = query_ref[g, h * 64 : (h + 1) * 64, :]
            query_full[(1 - h) * 64 : (2 - h) * 64, at] = jnp.zeros((64, 128), BF16)
            query_full[128:160, at] = query_ref[g, 128 + h * 32 : 160 + h * 32, :]
    best[...] = jnp.full(best.shape, LOW, F32)
    total[...] = jnp.zeros(total.shape, F32)
    acc[...] = jnp.zeros(acc.shape, F32)
    factor = SCALE * LOG2E

    def step(kb, masked):
        keys = key_rows[pl.ds(pl.multiple_of(kb * KEYS, KEYS), KEYS), :]

        def column(n, carry):
            first = pl.multiple_of(n * COLS, COLS)
            cols = pl.ds(first, COLS)
            scores = jnp.dot(keys, query_full[:, cols], preferred_element_type=F32)
            if masked:
                row = lax.broadcasted_iota(jnp.int32, (KEYS, 1), 0)
                key_at = (kb * (KEYS // 128) + row // 128) * queries + j * 128 + row % 128
                col = lax.broadcasted_iota(jnp.int32, (1, COLS), 1) + first
                query_at = z * queries + col % queries
                keep = key_at <= query_at
                scores = jnp.where(keep, scores, LOW)
            old = best[:, cols]
            new = jnp.maximum(old, jnp.max(scores, axis=0, keepdims=True))
            weights = jnp.exp2(scores * factor - new * factor)
            if masked:
                weights = jnp.where(keep, weights, 0.0)
            shrink = jnp.exp2((old - new) * factor)
            best[:, cols] = new
            total[:, cols] = total[:, cols] * shrink + jnp.sum(weights, axis=0, keepdims=True)
            head = first // queries
            values = value_cols[
                pl.ds(pl.multiple_of(head * 64, 64), 64),
                pl.ds(pl.multiple_of(kb * KEYS, KEYS), KEYS),
            ]
            acc[:, cols] = acc[:, cols] * shrink + jnp.dot(
                values, weights.astype(BF16), preferred_element_type=F32
            )
            return carry

        lax.fori_loop(0, width // COLS, column, 0)

    whole = z * 128 // KEYS

    def loop_body(kb, carry):
        step(kb, False)
        return carry

    lax.fori_loop(0, whole, loop_body, 0)
    step(whole, True)

    for h in range(2):
        span = slice(h * queries, (h + 1) * queries)
        sums = jnp.maximum(total[:, span], 1e-30)
        logsum = best[:, span] * SCALE + jnp.log(sums)
        part = logsum.astype(BF16)
        rest = logsum - part.astype(F32)
        middle = rest.astype(BF16)
        last = (rest - middle.astype(F32)).astype(BF16)
        mixed = (acc[:, span] / sums).astype(BF16)
        for g in range(groups):
            at = slice(g * 128, (g + 1) * 128)
            out_ref[g, h * 64 : (h + 1) * 64, :] = mixed[:, at]
            for i, piece in enumerate((part, middle, last)):
                out_ref[g, 128 + 16 * (2 * i + h) : 144 + 16 * (2 * i + h), :] = jnp.broadcast_to(
                    piece[:, at], (16, 128)
                )


OUT_ROWS = 224


def attend(place, keys, values, queries):
    blocks, groups = keys.shape[0], queries.shape[0]
    width = 2 * groups * 128
    vmem = pl.BlockSpec(memory_space=pltpu.VMEM)
    flops = 2 * blocks * 128 * width * (160 + 64)
    return pl.pallas_call(
        attention_kernel,
        out_shape=jax.ShapeDtypeStruct((groups, OUT_ROWS, 128), BF16),
        in_specs=[pl.BlockSpec(memory_space=pltpu.SMEM), vmem, vmem, vmem],
        out_specs=vmem,
        scratch_shapes=[
            pltpu.VMEM((blocks * 128, 160), BF16),
            pltpu.VMEM((128, blocks * 128), BF16),
            pltpu.VMEM((160, width), BF16),
            pltpu.VMEM((1, width), F32),
            pltpu.VMEM((1, width), F32),
            pltpu.VMEM((64, width), F32),
        ],
        cost_estimate=pl.CostEstimate(
            flops=flops, bytes_accessed=4_000_000, transcendentals=blocks * 128 * width
        ),
        name="attend",
    )(place, keys, values, queries)


def local(
    tokens,
    pre_gain,
    outer_gate,
    inner_gate,
    conv_input,
    conv_taps,
    query_down,
    latent_down,
    rotary_down,
    query_gain,
    latent_gain,
    query_up,
    query_rotary,
    key_up,
    value_up,
    conv_output,
    heads_output,
    post_gain,
):
    rows = tokens.shape[0]
    sp_index = lax.axis_index(SP)
    z = lax.axis_index("sp_0")
    j = lax.axis_index(GROUP)
    place = jnp.stack([z, j]).astype(jnp.int32)
    depth, channels = outer_gate.shape
    half = channels // 2

    gates = jnp.stack([outer_gate, inner_gate, conv_input], axis=1)
    gates = gates.reshape(depth, 3, 2, half).transpose(2, 0, 1, 3).reshape(2, depth, 3 * half)
    gates = exchange(gates, "sp_2").reshape(2 * depth, 3 * half)
    gates = copy_for_each(gates, "sp_0")
    gates = copy_for_each(gates, "sp_1")
    gates = gates.transpose(1, 0, 2, 3).reshape(-1, 3 * half)

    normed = rms_scale(tokens, pre_gain).astype(BF16)
    positions = sp_index * rows + jnp.arange(rows, dtype=jnp.int32)
    frequency = rope_theta ** (-jnp.arange(ROPE // 2, dtype=F32) / (ROPE // 2))
    angles = positions.astype(F32)[None, :] * frequency[:, None]
    cosine, sine = jnp.cos(angles), jnp.sin(angles)

    down = jnp.concatenate([latent_down, query_down], axis=1)
    latents = jnp.dot(normed, down, preferred_element_type=F32).astype(BF16)
    latents = copy_for_each(latents, "tp")
    n_latent = latent_down.shape[1]
    key_latent = jnp.moveaxis(latents[:, :, :n_latent], 0, 1).reshape(rows, -1)
    query_latent = jnp.moveaxis(latents[:, :, n_latent:], 0, 1).reshape(rows, -1)
    latent_normed = rms_scale(key_latent, latent_gain).astype(BF16)
    key_turned = rotate_rows(dot_t(normed, rotary_down), cosine, sine).astype(BF16)
    keys = jnp.concatenate([dot_t(latent_normed, key_up).astype(BF16), key_turned], axis=0)
    values = dot_t(latent_normed, value_up).astype(BF16)
    values = copy_for_each(values, "sp_0")
    query_normed = rms_scale(query_latent, query_gain).astype(BF16)
    query_nope = dot_t(query_normed, query_up).astype(BF16)
    turned = dot_t(query_normed, query_rotary).reshape(-1, ROPE, rows)
    turned = rotate_rows(turned, cosine, sine).astype(BF16).reshape(-1, rows)
    queries = copy_for_each(jnp.concatenate([query_nope, turned], axis=0), GROUP)
    keys = lax.all_gather(keys, "sp_0", axis=0, tiled=True).reshape(-1, *keys.shape)

    parts = attend(place, keys, values, queries)
    parts = exchange(parts, GROUP)

    other = lax.ppermute(gates, "sp_2", [(0, 1), (1, 0)])
    mine = jnp.dot(normed, gates, preferred_element_type=F32)
    other = jnp.dot(normed, other, preferred_element_type=F32)
    first_core = lax.axis_index("sp_2") == 0
    spread = [jnp.where(first_core, mine, other), jnp.where(first_core, other, mine)]
    outer_part, inner_part, signal = (
        jnp.concatenate([s[:, i * half : (i + 1) * half] for s in spread], axis=1) for i in range(3)
    )
    product = (inner_part * signal).astype(BF16)
    edge_rows = shifted(product[rows - (TAPS - 1) :], SP, 1)
    extended = jnp.concatenate([edge_rows, product], axis=0).astype(F32)
    convolved = extended[0:rows] * conv_taps[0]
    for offset in range(1, TAPS):
        convolved = convolved + extended[offset : offset + rows] * conv_taps[offset]
    conv_mixed = (outer_part * convolved).astype(BF16)
    conv_projected = jnp.dot(conv_mixed, conv_output, preferred_element_type=F32)

    groups = parts.shape[0]
    logs = parts[:, 128:].reshape(groups, 3, 2, 16, 128)[:, :, :, 0, :].astype(F32)
    logs = logs[:, 0] + (logs[:, 1] + logs[:, 2])
    top = jnp.max(logs, axis=0)
    share = jnp.exp(logs - top)
    share_sum = jnp.sum(share, axis=0)
    row_logsum = top + jnp.log(share_sum)
    share = share / share_sum
    mixed_parts = parts[:, :128].reshape(groups, 2, VDIM, 128).astype(F32)
    heads = jnp.sum(mixed_parts * share[:, :, None, :], axis=0).astype(BF16).reshape(-1, rows)
    heads_projected = lax.dot_general(
        heads, heads_output, (((0,), (0,)), ((), ())), preferred_element_type=F32
    )
    projected = (conv_projected + heads_projected).astype(BF16)
    tp = lax.axis_size("tp")
    arrived = exchange(projected.reshape(tp, rows // tp, -1), "tp")
    projected = arrived.astype(F32).sum(axis=0)
    mixed = rms_scale(projected, post_gain).astype(BF16)
    return (mixed, row_logsum)


def solution(mesh):
    split = Mesh(mesh.devices.reshape(16, 4, 2, mesh.shape["tp"]), ("sp_0", "sp_1", "sp_2", "tp"))
    return jax.shard_map(
        local,
        mesh=split,
        in_specs=(
            P(SP, None),
            P(),
            P(SP, "tp"),
            P(SP, "tp"),
            P(SP, "tp"),
            P(None, "tp"),
            P(None, "tp"),
            P(None, "tp"),
            P(),
            P(),
            P(),
            P(None, "tp"),
            P(None, "tp"),
            P(None, "tp"),
            P(None, "tp"),
            P("tp", None),
            P("tp", None),
            P(),
        ),
        out_specs=(P(SP_TP, None), P("tp", SP)),
        check_vma=False,
    )
```

```python
import math

import jax
import jax.numpy as jnp
from jax import lax
from jax.experimental import pallas as pl
from jax.experimental.pallas import tpu as pltpu
from jax.sharding import Mesh
from jax.sharding import PartitionSpec as P

NOPE = 64
ROPE = 32
VDIM = 64
TAPS = 3
SP = ("far", "pair", "x", "core")
SP_TP = ("far", "pair", "x", "core", "tp")
Z = ("far", "pair")
GROUP = ("pair", "x", "core")

eps = 1e-06
rope_theta = 500000.0
SCALE = (NOPE + ROPE) ** (-0.5)
LOG2E = math.log2(math.e)
LOW = -1e30
BF16 = jnp.bfloat16
F32 = jnp.float32


def copy_for_each(array, axis):
    copies = jnp.broadcast_to(array, (lax.axis_size(axis), *array.shape))
    return lax.all_to_all(copies, axis, split_axis=0, concat_axis=0, tiled=True)


def ring_gather(array, axis):
    count, here = lax.axis_size(axis), lax.axis_index(axis)
    whole = jnp.zeros((array.shape[0], count, *array.shape[1:]), array.dtype)
    for k in range(count):
        block = array
        if k:
            block = lax.ppermute(array, axis, [(i, (i + k) % count) for i in range(count)])
        at = (0, (here + count - k) % count) + (0,) * (array.ndim - 1)
        whole = lax.dynamic_update_slice(whole, block[:, None], at)
    return whole


def exchange(array, axis):
    return lax.all_to_all(array, axis, split_axis=0, concat_axis=0, tiled=True)


def shifted(value, axis, steps):
    count = lax.axis_size(axis)
    first, last = (max(0, -steps), min(count, count - steps))
    return lax.ppermute(value, axis, [(source, source + steps) for source in range(first, last)])


def rms_scale(values, scale_row):
    widened = values.astype(F32)
    return (
        widened * lax.rsqrt(jnp.mean(widened * widened, axis=-1, keepdims=True) + eps) * scale_row
    )


def dot_t(values, weights):
    return lax.dot_general(weights, values, (((0,), (1,)), ((), ())), preferred_element_type=F32)


def rotate_rows(values, cosine, sine):
    half = values.shape[-2] // 2
    leading = values[..., :half, :]
    trailing = values[..., half:, :]
    return jnp.concatenate(
        [leading * cosine - trailing * sine, trailing * cosine + leading * sine], axis=-2
    )


KEYS = 256
COLS = 512


def attention_kernel(
    place, held_ref, query_ref, out_ref, key_rows, value_cols, query_full, best, total, acc
):
    z = place[0]
    j = place[1]
    blocks = held_ref.shape[0]
    groups = query_ref.shape[0]
    queries = groups * 128
    width = 2 * queries
    for b in range(blocks):
        key_rows[b * 128 : (b + 1) * 128, :] = held_ref[b, 0:160, :].T
        value_cols[:, b * 128 : (b + 1) * 128] = held_ref[b, 160:288, :]
    for h in range(2):
        for g in range(groups):
            at = slice(h * queries + g * 128, h * queries + (g + 1) * 128)
            query_full[h * 64 : (h + 1) * 64, at] = query_ref[g, h * 64 : (h + 1) * 64, :]
            query_full[(1 - h) * 64 : (2 - h) * 64, at] = jnp.zeros((64, 128), BF16)
            query_full[128:160, at] = query_ref[g, 128 + h * 32 : 160 + h * 32, :]
    best[...] = jnp.full(best.shape, LOW, F32)
    total[...] = jnp.zeros(total.shape, F32)
    acc[...] = jnp.zeros(acc.shape, F32)
    factor = SCALE * LOG2E

    def step(kb, masked):
        keys = key_rows[pl.ds(pl.multiple_of(kb * KEYS, KEYS), KEYS), :]

        for n in range(width // COLS):
            first = n * COLS
            cols = slice(first, first + COLS)
            scores = jnp.dot(keys, query_full[:, cols], preferred_element_type=F32)
            if masked:
                row = lax.broadcasted_iota(jnp.int32, (KEYS, 1), 0)
                key_at = (kb * (KEYS // 128) + row // 128) * queries + j * 128 + row % 128
                col = lax.broadcasted_iota(jnp.int32, (1, COLS), 1) + first % queries
                keep = key_at <= z * queries + col
                scores = jnp.where(keep, scores, LOW)
            old = best[:, cols]
            new = jnp.maximum(old, jnp.max(scores, axis=0, keepdims=True))
            weights = jnp.exp2(scores * factor - new * factor)
            if masked:
                weights = jnp.where(keep, weights, 0.0)
            shrink = jnp.exp2((old - new) * factor)
            best[:, cols] = new
            total[:, cols] = total[:, cols] * shrink + jnp.sum(weights, axis=0, keepdims=True)
            head = first // queries
            values = value_cols[
                head * 64 : (head + 1) * 64, pl.ds(pl.multiple_of(kb * KEYS, KEYS), KEYS)
            ]
            acc[:, cols] = acc[:, cols] * shrink + jnp.dot(
                values, weights.astype(BF16), preferred_element_type=F32
            )

    whole = z * 128 // KEYS

    def loop_body(kb, carry):
        step(kb, False)
        return carry

    lax.fori_loop(0, whole, loop_body, 0)
    step(whole, True)

    for h in range(2):
        span = slice(h * queries, (h + 1) * queries)
        sums = jnp.maximum(total[:, span], 1e-30)
        logsum = best[:, span] * SCALE + jnp.log(sums)
        part = logsum.astype(BF16)
        rest = logsum - part.astype(F32)
        middle = rest.astype(BF16)
        last = (rest - middle.astype(F32)).astype(BF16)
        mixed = (acc[:, span] / sums).astype(BF16)
        for g in range(groups):
            at = slice(g * 128, (g + 1) * 128)
            out_ref[g, h * 64 : (h + 1) * 64, :] = mixed[:, at]
            for i, piece in enumerate((part, middle, last)):
                out_ref[g, 128 + 16 * (2 * i + h) : 144 + 16 * (2 * i + h), :] = jnp.broadcast_to(
                    piece[:, at], (16, 128)
                )


OUT_ROWS = 224


def attend(place, held, queries):
    blocks, groups = held.shape[0], queries.shape[0]
    width = 2 * groups * 128
    vmem = pl.BlockSpec(memory_space=pltpu.VMEM)
    flops = 2 * blocks * 128 * width * (160 + 64)
    return pl.pallas_call(
        attention_kernel,
        out_shape=jax.ShapeDtypeStruct((groups, OUT_ROWS, 128), BF16),
        in_specs=[pl.BlockSpec(memory_space=pltpu.SMEM), vmem, vmem],
        out_specs=vmem,
        scratch_shapes=[
            pltpu.VMEM((blocks * 128, 160), BF16),
            pltpu.VMEM((128, blocks * 128), BF16),
            pltpu.VMEM((160, width), BF16),
            pltpu.VMEM((1, width), F32),
            pltpu.VMEM((1, width), F32),
            pltpu.VMEM((64, width), F32),
        ],
        cost_estimate=pl.CostEstimate(
            flops=flops, bytes_accessed=4_000_000, transcendentals=blocks * 128 * width
        ),
        name="attend",
    )(place, held, queries)


def layer(
    tokens,
    pre_gain,
    outer_gate,
    inner_gate,
    conv_input,
    conv_taps,
    query_down,
    latent_down,
    rotary_down,
    query_gain,
    latent_gain,
    query_up,
    query_rotary,
    key_up,
    value_up,
    conv_output,
    heads_output,
    post_gain,
):
    rows = tokens.shape[0]
    sp_index = lax.axis_index(SP)
    place = jnp.stack([lax.axis_index("far"), lax.axis_index(GROUP)]).astype(jnp.int32)
    core = lax.axis_index("core")

    gates = jnp.concatenate([outer_gate, inner_gate, conv_input], axis=1)
    half = gates.shape[1] // 2
    gates = lax.all_gather(gates, "core", axis=0, tiled=True)
    gates = jnp.where(core == 0, gates[:, :half], gates[:, half:])
    gates = copy_for_each(gates, Z)
    gates = ring_gather(gates, "x").reshape(-1, half)
    gates_other = lax.ppermute(gates, "core", [(0, 1), (1, 0)])

    normed = rms_scale(tokens, pre_gain).astype(BF16)
    down = jnp.concatenate([latent_down, query_down], axis=1)
    latents = jnp.dot(normed, down, preferred_element_type=F32).astype(BF16)
    latents = lax.all_gather(latents, "tp", axis=0)

    positions = sp_index * rows + jnp.arange(rows, dtype=jnp.int32)
    frequency = rope_theta ** (-jnp.arange(ROPE // 2, dtype=F32) / (ROPE // 2))
    angles = positions.astype(F32)[None, :] * frequency[:, None]
    cosine, sine = jnp.cos(angles), jnp.sin(angles)
    key_turned = rotate_rows(dot_t(normed, rotary_down), cosine, sine).astype(BF16)

    n_latent = latent_down.shape[1]
    key_latent = jnp.moveaxis(latents[:, :, :n_latent], 0, 1).reshape(rows, -1)
    query_latent = jnp.moveaxis(latents[:, :, n_latent:], 0, 1).reshape(rows, -1)
    latent_normed = rms_scale(key_latent, latent_gain).astype(BF16)
    query_normed = rms_scale(query_latent, query_gain).astype(BF16)
    query_nope = dot_t(query_normed, query_up).astype(BF16)
    turned = dot_t(query_normed, query_rotary).reshape(-1, ROPE, rows)
    turned = rotate_rows(turned, cosine, sine).astype(BF16).reshape(-1, rows)
    queries = jnp.concatenate([query_nope, turned], axis=0)
    queries = copy_for_each(queries, GROUP)
    held = jnp.concatenate(
        [
            dot_t(latent_normed, key_up).astype(BF16),
            key_turned,
            dot_t(latent_normed, value_up).astype(BF16),
        ],
        axis=0,
    )
    held = lax.all_gather(held, "far", axis=0, tiled=True).reshape(-1, *held.shape)

    parts = attend(place, held, queries)
    parts = exchange(parts, GROUP)

    mine = jnp.dot(normed, gates, preferred_element_type=F32)
    other = jnp.dot(normed, gates_other, preferred_element_type=F32)
    spread = [jnp.where(core == 0, mine, other), jnp.where(core == 0, other, mine)]
    outer_part, inner_part, signal = jnp.split(jnp.concatenate(spread, axis=1), 3, axis=1)
    product = (inner_part * signal).astype(BF16)
    edge_rows = shifted(product[rows - (TAPS - 1) :], SP, 1)
    extended = jnp.concatenate([edge_rows, product], axis=0).astype(F32)
    convolved = extended[0:rows] * conv_taps[0]
    for offset in range(1, TAPS):
        convolved = convolved + extended[offset : offset + rows] * conv_taps[offset]
    conv_mixed = (outer_part * convolved).astype(BF16)
    conv_projected = jnp.dot(conv_mixed, conv_output, preferred_element_type=F32)

    groups = parts.shape[0]
    logs = parts[:, 128:].reshape(groups, 3, 2, 16, 128)[:, :, :, 0, :].astype(F32)
    logs = logs[:, 0] + (logs[:, 1] + logs[:, 2])
    top = jnp.max(logs, axis=0)
    share = jnp.exp(logs - top)
    share_sum = jnp.sum(share, axis=0)
    row_logsum = top + jnp.log(share_sum)
    share = share / share_sum
    mixed_parts = parts[:, :128].reshape(groups, 2, VDIM, 128).astype(F32)
    heads = jnp.sum(mixed_parts * share[:, :, None, :], axis=0).astype(BF16).reshape(-1, rows)
    heads_projected = lax.dot_general(
        heads, heads_output, (((0,), (0,)), ((), ())), preferred_element_type=F32
    )
    projected = (conv_projected + heads_projected).astype(BF16)
    tp = lax.axis_size("tp")
    arrived = exchange(projected.reshape(tp, rows // tp, -1), "tp")
    projected = arrived.astype(F32).sum(axis=0)
    mixed = rms_scale(projected, post_gain).astype(BF16)
    return (mixed, row_logsum)


def solution(mesh):
    split = Mesh(mesh.devices.reshape(8, 2, 4, 2, mesh.shape["tp"]), SP_TP)
    return jax.shard_map(
        layer,
        mesh=split,
        in_specs=(
            P(SP, None),
            P(),
            P(SP, "tp"),
            P(SP, "tp"),
            P(SP, "tp"),
            P(None, "tp"),
            P(None, "tp"),
            P(None, "tp"),
            P(),
            P(),
            P(),
            P(None, "tp"),
            P(None, "tp"),
            P(None, "tp"),
            P(None, "tp"),
            P("tp", None),
            P("tp", None),
            P(),
        ),
        out_specs=(P(SP_TP, None), P("tp", SP)),
        check_vma=False,
    )
```

```python
import math

import jax
import jax.numpy as jnp
from jax import lax
from jax.experimental import pallas as pl
from jax.experimental.pallas import tpu as pltpu
from jax.sharding import Mesh
from jax.sharding import PartitionSpec as P

NOPE = 64
ROPE = 32
VDIM = 64
TAPS = 3
SP = ("far", "pair", "x", "core")
SP_TP = ("far", "pair", "x", "core", "tp")
Z = ("far", "pair")
GROUP = ("pair", "x", "core")

eps = 1e-06
rope_theta = 500000.0
SCALE = (NOPE + ROPE) ** (-0.5)
LOG2E = math.log2(math.e)
LOW = -1e30
BF16 = jnp.bfloat16
F32 = jnp.float32


def copy_for_each(array, axis):
    copies = jnp.broadcast_to(array, (lax.axis_size(axis), *array.shape))
    return lax.all_to_all(copies, axis, split_axis=0, concat_axis=0, tiled=True)


def weight_rows(joint, depth, wide, cores):
    rows = joint[:, 2 * QUERY_ROWS :].reshape(wide, cores, -1, 6, depth, 128)
    rows = rows.transpose(2, 0, 1, 4, 3, 5)
    return rows.reshape(-1, 6 * 128)


def exchange(array, axis):
    return lax.all_to_all(array, axis, split_axis=0, concat_axis=0, tiled=True)


def shifted(value, axis, steps):
    count = lax.axis_size(axis)
    first, last = (max(0, -steps), min(count, count - steps))
    return lax.ppermute(value, axis, [(source, source + steps) for source in range(first, last)])


def rms_scale(values, scale_row):
    widened = values.astype(F32)
    return (
        widened * lax.rsqrt(jnp.mean(widened * widened, axis=-1, keepdims=True) + eps) * scale_row
    )


def dot_t(values, weights):
    return lax.dot_general(weights, values, (((0,), (1,)), ((), ())), preferred_element_type=F32)


def rotate_rows(values, cosine, sine):
    half = values.shape[-2] // 2
    leading = values[..., :half, :]
    trailing = values[..., half:, :]
    return jnp.concatenate(
        [leading * cosine - trailing * sine, trailing * cosine + leading * sine], axis=-2
    )


KEYS = 256
QUERY_ROWS = 192
COLS = 512


def attention_kernel(
    place, held_ref, query_ref, out_ref, key_rows, value_cols, query_full, best, total, acc
):
    z = place[0]
    j = place[1]
    blocks = held_ref.shape[0]
    near = query_ref.shape[0]
    groups = 2 * near
    queries = groups * 128
    width = 2 * queries
    for b in range(blocks):
        key_rows[b * 128 : (b + 1) * 128, :] = held_ref[b, 0:160, :].T
        value_cols[:, b * 128 : (b + 1) * 128] = held_ref[b, 160:288, :]
    for h in range(2):
        for g in range(groups):
            at = slice(h * queries + g * 128, h * queries + (g + 1) * 128)
            from_row = g // near * QUERY_ROWS
            query_full[h * 64 : (h + 1) * 64, at] = query_ref[
                g % near, from_row + h * 64 : from_row + (h + 1) * 64, :
            ]
            query_full[(1 - h) * 64 : (2 - h) * 64, at] = jnp.zeros((64, 128), BF16)
            query_full[128:160, at] = query_ref[
                g % near, from_row + 128 + h * 32 : from_row + 160 + h * 32, :
            ]
    best[...] = jnp.full(best.shape, LOW, F32)
    total[...] = jnp.zeros(total.shape, F32)
    acc[...] = jnp.zeros(acc.shape, F32)
    factor = SCALE * LOG2E

    def step(kb, masked):
        keys = key_rows[pl.ds(pl.multiple_of(kb * KEYS, KEYS), KEYS), :]

        for n in range(width // COLS):
            first = n * COLS
            cols = slice(first, first + COLS)
            scores = jnp.dot(keys, query_full[:, cols], preferred_element_type=F32)
            if masked:
                row = lax.broadcasted_iota(jnp.int32, (KEYS, 1), 0)
                key_at = (kb * (KEYS // 128) + row // 128) * queries + j * 128 + row % 128
                col = lax.broadcasted_iota(jnp.int32, (1, COLS), 1) + first % queries
                keep = key_at <= z * queries + col
                scores = jnp.where(keep, scores, LOW)
            old = best[:, cols]
            new = jnp.maximum(old, jnp.max(scores, axis=0, keepdims=True))
            weights = jnp.exp2(scores * factor - new * factor)
            if masked:
                weights = jnp.where(keep, weights, 0.0)
            shrink = jnp.exp2((old - new) * factor)
            best[:, cols] = new
            total[:, cols] = total[:, cols] * shrink + jnp.sum(weights, axis=0, keepdims=True)
            head = first // queries
            values = value_cols[
                head * 64 : (head + 1) * 64, pl.ds(pl.multiple_of(kb * KEYS, KEYS), KEYS)
            ]
            acc[:, cols] = acc[:, cols] * shrink + jnp.dot(
                values, weights.astype(BF16), preferred_element_type=F32
            )

    whole = z * 128 // KEYS

    def loop_body(kb, carry):
        step(kb, False)
        return carry

    lax.fori_loop(0, whole, loop_body, 0)
    step(whole, True)

    for h in range(2):
        span = slice(h * queries, (h + 1) * queries)
        sums = jnp.maximum(total[:, span], 1e-30)
        logsum = best[:, span] * SCALE + jnp.log(sums)
        part = logsum.astype(BF16)
        rest = logsum - part.astype(F32)
        middle = rest.astype(BF16)
        last = (rest - middle.astype(F32)).astype(BF16)
        mixed = (acc[:, span] / sums).astype(BF16)
        for g in range(groups):
            at = slice(g * 128, (g + 1) * 128)
            out_ref[g, h * 64 : (h + 1) * 64, :] = mixed[:, at]
            for i, piece in enumerate((part, middle, last)):
                out_ref[g, 128 + 16 * (2 * i + h) : 144 + 16 * (2 * i + h), :] = jnp.broadcast_to(
                    piece[:, at], (16, 128)
                )


OUT_ROWS = 224


def attend(place, held, joint):
    blocks, groups = held.shape[0], 2 * joint.shape[0]
    width = 2 * groups * 128
    flops = 2 * blocks * 128 * width * (160 + 64)
    return pl.pallas_call(
        attention_kernel,
        out_shape=jax.ShapeDtypeStruct((groups, OUT_ROWS, 128), BF16),
        grid=(1,),
        in_specs=[
            pl.BlockSpec(memory_space=pltpu.SMEM),
            pl.BlockSpec(held.shape, lambda i: (0, 0, 0)),
            pl.BlockSpec((groups // 2, 2 * QUERY_ROWS, 128), lambda i: (0, 0, 0)),
        ],
        out_specs=pl.BlockSpec((groups, OUT_ROWS, 128), lambda i: (0, 0, 0)),
        scratch_shapes=[
            pltpu.VMEM((blocks * 128, 160), BF16),
            pltpu.VMEM((128, blocks * 128), BF16),
            pltpu.VMEM((160, width), BF16),
            pltpu.VMEM((1, width), F32),
            pltpu.VMEM((1, width), F32),
            pltpu.VMEM((64, width), F32),
        ],
        cost_estimate=pl.CostEstimate(
            flops=flops, bytes_accessed=4_000_000, transcendentals=blocks * 128 * width
        ),
        name="attend",
    )(place, held, joint)


def layer(
    tokens,
    pre_gain,
    outer_gate,
    inner_gate,
    conv_input,
    conv_taps,
    query_down,
    latent_down,
    rotary_down,
    query_gain,
    latent_gain,
    query_up,
    query_rotary,
    key_up,
    value_up,
    conv_output,
    heads_output,
    post_gain,
):
    rows = tokens.shape[0]
    sp_index = lax.axis_index(SP)
    place = jnp.stack([lax.axis_index("far"), lax.axis_index(GROUP)]).astype(jnp.int32)
    core = lax.axis_index("core")

    depth = outer_gate.shape[0]
    gates = jnp.concatenate([outer_gate, inner_gate, conv_input], axis=1)
    gates = gates.reshape(depth, -1, 128).swapaxes(0, 1).reshape(-1, 128)
    gates = copy_for_each(gates, Z)

    normed = rms_scale(tokens, pre_gain).astype(BF16)
    down = jnp.concatenate([latent_down, query_down], axis=1)
    latents = jnp.dot(normed, down, preferred_element_type=F32).astype(BF16)
    latents = lax.all_gather(latents, "tp", axis=0)

    positions = sp_index * rows + jnp.arange(rows, dtype=jnp.int32)
    frequency = rope_theta ** (-jnp.arange(ROPE // 2, dtype=F32) / (ROPE // 2))
    angles = positions.astype(F32)[None, :] * frequency[:, None]
    cosine, sine = jnp.cos(angles), jnp.sin(angles)
    key_turned = rotate_rows(dot_t(normed, rotary_down), cosine, sine).astype(BF16)

    n_latent = latent_down.shape[1]
    key_latent = jnp.moveaxis(latents[:, :, :n_latent], 0, 1).reshape(rows, -1)
    query_latent = jnp.moveaxis(latents[:, :, n_latent:], 0, 1).reshape(rows, -1)
    latent_normed = rms_scale(key_latent, latent_gain).astype(BF16)
    query_normed = rms_scale(query_latent, query_gain).astype(BF16)
    query_nope = dot_t(query_normed, query_up).astype(BF16)
    turned = dot_t(query_normed, query_rotary).reshape(-1, ROPE, rows)
    turned = rotate_rows(turned, cosine, sine).astype(BF16).reshape(-1, rows)
    queries = jnp.concatenate([query_nope, turned], axis=0)
    queries_other = lax.ppermute(queries, "pair", [(0, 1), (1, 0)])
    first_of_pair = lax.axis_index("pair") == 0
    both = [
        jnp.where(first_of_pair, queries, queries_other),
        jnp.where(first_of_pair, queries_other, queries),
    ]
    _, wide, cores = (lax.axis_size(name) for name in GROUP)
    halves = gates.reshape(cores, -1, 128)
    both = jnp.broadcast_to(jnp.concatenate(both, axis=0), (wide, cores, 2 * QUERY_ROWS, 128))
    halves = jnp.broadcast_to(halves, (wide, *halves.shape))
    sent = jnp.concatenate([both, halves], axis=2)
    joint = exchange(sent.reshape(-1, *sent.shape[2:]), GROUP[1:])
    joint_other = lax.ppermute(joint, "core", [(0, 1), (1, 0)])
    held = jnp.concatenate(
        [
            dot_t(latent_normed, key_up).astype(BF16),
            key_turned,
            dot_t(latent_normed, value_up).astype(BF16),
        ],
        axis=0,
    )
    held = lax.all_gather(held, "far", axis=0, tiled=True).reshape(-1, *held.shape)

    parts = attend(place, held, joint)
    parts = exchange(parts, GROUP)

    mine, other = (weight_rows(whole, depth, wide, cores) for whole in (joint, joint_other))
    low, high = jnp.split(normed, 2, axis=1)
    spread = jnp.dot(jnp.where(core == 0, low, high), mine, preferred_element_type=F32)
    spread += jnp.dot(jnp.where(core == 0, high, low), other, preferred_element_type=F32)
    outer_part, inner_part, signal = jnp.split(spread, 3, axis=1)
    product = (inner_part * signal).astype(BF16)
    edge_rows = shifted(product[rows - (TAPS - 1) :], SP, 1)
    extended = jnp.concatenate([edge_rows, product], axis=0).astype(F32)
    convolved = extended[0:rows] * conv_taps[0]
    for offset in range(1, TAPS):
        convolved = convolved + extended[offset : offset + rows] * conv_taps[offset]
    conv_mixed = (outer_part * convolved).astype(BF16)
    conv_projected = jnp.dot(conv_mixed, conv_output, preferred_element_type=F32)

    groups = parts.shape[0]
    logs = parts[:, 128:].reshape(groups, 3, 2, 16, 128)[:, :, :, 0, :].astype(F32)
    logs = logs[:, 0] + (logs[:, 1] + logs[:, 2])
    top = jnp.max(logs, axis=0)
    share = jnp.exp(logs - top)
    share_sum = jnp.sum(share, axis=0)
    row_logsum = top + jnp.log(share_sum)
    share = share / share_sum
    mixed_parts = parts[:, :128].reshape(groups, 2, VDIM, 128).astype(F32)
    heads = jnp.sum(mixed_parts * share[:, :, None, :], axis=0).astype(BF16).reshape(-1, rows)
    heads_projected = lax.dot_general(
        heads, heads_output, (((0,), (0,)), ((), ())), preferred_element_type=F32
    )
    projected = (conv_projected + heads_projected).astype(BF16)
    tp = lax.axis_size("tp")
    arrived = exchange(projected.reshape(tp, rows // tp, -1), "tp")
    projected = arrived.astype(F32).sum(axis=0)
    mixed = rms_scale(projected, post_gain).astype(BF16)
    return (mixed, row_logsum)


def solution(mesh):
    split = Mesh(mesh.devices.reshape(8, 2, 4, 2, mesh.shape["tp"]), SP_TP)
    return jax.shard_map(
        layer,
        mesh=split,
        in_specs=(
            P(SP, None),
            P(),
            P(SP, "tp"),
            P(SP, "tp"),
            P(SP, "tp"),
            P(None, "tp"),
            P(None, "tp"),
            P(None, "tp"),
            P(),
            P(),
            P(),
            P(None, "tp"),
            P(None, "tp"),
            P(None, "tp"),
            P(None, "tp"),
            P("tp", None),
            P("tp", None),
            P(),
        ),
        out_specs=(P(SP_TP, None), P("tp", SP)),
        check_vma=False,
    )
```

```python
import math

import jax
import jax.numpy as jnp
from jax import lax
from jax.experimental import pallas as pl
from jax.experimental.pallas import tpu as pltpu
from jax.sharding import Mesh
from jax.sharding import PartitionSpec as P

NOPE = 64
ROPE = 32
VDIM = 64
TAPS = 3
SP = ("far", "pair", "x", "core")
SP_TP = ("far", "pair", "x", "core", "tp")
Z = ("far", "pair")
GROUP = ("pair", "x", "core")

eps = 1e-06
rope_theta = 500000.0
SCALE = (NOPE + ROPE) ** (-0.5)
LOG2E = math.log2(math.e)
LOW = -1e30
BF16 = jnp.bfloat16
F32 = jnp.float32


def copy_for_each(array, axis):
    copies = jnp.broadcast_to(array, (lax.axis_size(axis), *array.shape))
    return lax.all_to_all(copies, axis, split_axis=0, concat_axis=0, tiled=True)


def weight_rows(joint, depth, wide, cores):
    rows = joint[:, 2 * QUERY_ROWS :].reshape(wide, cores, -1, 6, depth, 128)
    rows = rows.transpose(2, 0, 1, 4, 3, 5)
    return rows.reshape(-1, 6 * 128)


def exchange(array, axis):
    return lax.all_to_all(array, axis, split_axis=0, concat_axis=0, tiled=True)


def shifted(value, axis, steps):
    count = lax.axis_size(axis)
    first, last = (max(0, -steps), min(count, count - steps))
    return lax.ppermute(value, axis, [(source, source + steps) for source in range(first, last)])


def rms_scale(values, scale_row):
    widened = values.astype(F32)
    return (
        widened * lax.rsqrt(jnp.mean(widened * widened, axis=-1, keepdims=True) + eps) * scale_row
    )


def dot_t(values, weights):
    return lax.dot_general(weights, values, (((0,), (1,)), ((), ())), preferred_element_type=F32)


def rotate_rows(values, cosine, sine):
    half = values.shape[-2] // 2
    leading = values[..., :half, :]
    trailing = values[..., half:, :]
    return jnp.concatenate(
        [leading * cosine - trailing * sine, trailing * cosine + leading * sine], axis=-2
    )


COLS = 256
QUERY_ROWS = 192
PART_ROWS = 144
FLOOR = -1e29


def attention_kernel(place, held_ref, query_ref, out_ref, key_rows, value_cols, query_full):
    far, here = place[0], place[1]
    blocks = held_ref.shape[0]
    near = query_ref.shape[0]
    groups = 2 * near
    queries = groups * 128
    for b in range(blocks):
        key_rows[b * 128 : (b + 1) * 128, :] = held_ref[b, 0:160, :].T
        value_cols[:, b * 128 : (b + 1) * 128] = held_ref[b, 160:288, :]
    for h in range(2):
        for g in range(groups):
            at = slice(h * queries + g * 128, h * queries + (g + 1) * 128)
            first = g // near * QUERY_ROWS
            query_full[h * 64 : (h + 1) * 64, at] = query_ref[
                g % near, first + h * 64 : first + (h + 1) * 64, :
            ]
            query_full[(1 - h) * 64 : (2 - h) * 64, at] = jnp.zeros((64, 128), BF16)
            query_full[128:160, at] = query_ref[
                g % near, first + 128 + h * 32 : first + 160 + h * 32, :
            ]
    factor = SCALE * LOG2E
    row = lax.broadcasted_iota(jnp.int32, (blocks * 128, 1), 0)
    key_at = row // 128 * queries + here * 128 + row % 128 - far * queries

    def score(first):
        return jnp.dot(
            key_rows[...], query_full[:, first : first + COLS], preferred_element_type=F32
        )

    def soften(first, scores):
        col = lax.broadcasted_iota(jnp.int32, (1, COLS), 1) + first % queries
        scores = jnp.where(key_at <= col, scores, LOW)
        best = jnp.maximum(jnp.max(scores, axis=0, keepdims=True), FLOOR)
        weights = jnp.exp2(scores * factor - best * factor)
        total = jnp.maximum(jnp.sum(weights, axis=0, keepdims=True), 1e-30)
        return weights.astype(BF16), total, best * SCALE + jnp.log(total)

    logs = {}

    def mix(first, weights, total, logsum):
        h = first // queries
        mixed = jnp.dot(
            value_cols[h * 64 : (h + 1) * 64, :], weights, preferred_element_type=F32
        )
        mixed = (mixed * (1.0 / total)).astype(BF16)
        high = logsum.astype(BF16).astype(F32)
        middle = (logsum - high).astype(BF16).astype(F32)
        low = logsum - high - middle
        tail = jnp.concatenate([high, middle, low, jnp.zeros((5, COLS), F32)], axis=0)
        for i in range(COLS // 128):
            g = first % queries // 128 + i
            at = slice(i * 128, (i + 1) * 128)
            out_ref[g, h * 64 : (h + 1) * 64, :] = mixed[:, at]
            if h == 0:
                logs[g] = tail[:, at]
            else:
                both = jnp.concatenate([logs.pop(g), tail[:, at]], axis=0)
                out_ref[g, 128:PART_ROWS, :] = both.astype(BF16)

    tiles = 2 * queries // COLS
    scores, softened = {}, {}
    for n in range(tiles + 2):
        if 0 <= n - 1 < tiles:
            softened[n - 1] = soften((n - 1) * COLS, scores.pop(n - 1))
        if n < tiles:
            scores[n] = score(n * COLS)
        if 0 <= n - 2 < tiles:
            mix((n - 2) * COLS, *softened.pop(n - 2))


def attend(place, held, joint):
    blocks, groups = held.shape[0], 2 * joint.shape[0]
    width = 2 * groups * 128
    return pl.pallas_call(
        attention_kernel,
        out_shape=jax.ShapeDtypeStruct((groups, PART_ROWS, 128), BF16),
        grid=(1,),
        in_specs=[
            pl.BlockSpec(memory_space=pltpu.SMEM),
            pl.BlockSpec(held.shape, lambda i: (0, 0, 0)),
            pl.BlockSpec((groups // 2, 2 * QUERY_ROWS, 128), lambda i: (0, 0, 0)),
        ],
        out_specs=pl.BlockSpec((groups, PART_ROWS, 128), lambda i: (0, 0, 0)),
        scratch_shapes=[
            pltpu.VMEM((blocks * 128, 160), BF16),
            pltpu.VMEM((128, blocks * 128), BF16),
            pltpu.VMEM((160, width), BF16),
        ],
        cost_estimate=pl.CostEstimate(
            flops=2 * blocks * 128 * width * (160 + 64),
            bytes_accessed=2_000_000,
            transcendentals=blocks * 128 * width,
        ),
        name="attend",
    )(place, held, joint)


def layer(
    tokens,
    pre_gain,
    outer_gate,
    inner_gate,
    conv_input,
    conv_taps,
    query_down,
    latent_down,
    rotary_down,
    query_gain,
    latent_gain,
    query_up,
    query_rotary,
    key_up,
    value_up,
    conv_output,
    heads_output,
    post_gain,
):
    rows = tokens.shape[0]
    sp_index = lax.axis_index(SP)
    place = jnp.stack([lax.axis_index("far"), lax.axis_index(GROUP)]).astype(jnp.int32)
    core = lax.axis_index("core")

    depth = outer_gate.shape[0]
    gates = jnp.concatenate([outer_gate, inner_gate, conv_input], axis=1)
    gates = gates.reshape(depth, -1, 128).swapaxes(0, 1).reshape(-1, 128)
    gates = copy_for_each(gates, Z)

    edge = shifted(tokens[rows - (TAPS - 1) :], SP, 1)

    normed = rms_scale(tokens, pre_gain).astype(BF16)
    down = jnp.concatenate([latent_down, query_down], axis=1)
    latents = jnp.dot(normed, down, preferred_element_type=F32).astype(BF16)
    latents = lax.all_gather(latents, "tp", axis=0)

    positions = sp_index * rows + jnp.arange(rows, dtype=jnp.int32)
    frequency = rope_theta ** (-jnp.arange(ROPE // 2, dtype=F32) / (ROPE // 2))
    angles = positions.astype(F32)[None, :] * frequency[:, None]
    cosine, sine = jnp.cos(angles), jnp.sin(angles)
    key_turned = rotate_rows(dot_t(normed, rotary_down), cosine, sine).astype(BF16)

    n_latent = latent_down.shape[1]
    key_latent = jnp.moveaxis(latents[:, :, :n_latent], 0, 1).reshape(rows, -1)
    query_latent = jnp.moveaxis(latents[:, :, n_latent:], 0, 1).reshape(rows, -1)
    latent_normed = rms_scale(key_latent, latent_gain).astype(BF16)
    query_normed = rms_scale(query_latent, query_gain).astype(BF16)
    query_nope = dot_t(query_normed, query_up).astype(BF16)
    turned = dot_t(query_normed, query_rotary).reshape(-1, ROPE, rows)
    turned = rotate_rows(turned, cosine, sine).astype(BF16).reshape(-1, rows)
    queries = jnp.concatenate([query_nope, turned], axis=0)
    queries_other = lax.ppermute(queries, "pair", [(0, 1), (1, 0)])
    first_of_pair = lax.axis_index("pair") == 0
    both = [
        jnp.where(first_of_pair, queries, queries_other),
        jnp.where(first_of_pair, queries_other, queries),
    ]
    _, wide, cores = (lax.axis_size(name) for name in GROUP)
    halves = gates.reshape(cores, -1, 128)
    both = jnp.broadcast_to(jnp.concatenate(both, axis=0), (wide, cores, 2 * QUERY_ROWS, 128))
    halves = jnp.broadcast_to(halves, (wide, *halves.shape))
    sent = jnp.concatenate([both, halves], axis=2)
    joint = exchange(sent.reshape(-1, *sent.shape[2:]), GROUP[1:])
    joint_other = lax.ppermute(joint, "core", [(0, 1), (1, 0)])
    held = jnp.concatenate(
        [
            dot_t(latent_normed, key_up).astype(BF16),
            key_turned,
            dot_t(latent_normed, value_up).astype(BF16),
        ],
        axis=0,
    )
    held = lax.all_gather(held, "far", axis=0, tiled=True).reshape(-1, *held.shape)

    parts = attend(place, held, joint)
    parts = exchange(parts, GROUP)

    mine, other = (weight_rows(whole, depth, wide, cores) for whole in (joint, joint_other))
    lead = 16
    edge = jnp.pad(edge, ((lead - (TAPS - 1), 0), (0, 0)))
    edge = rms_scale(edge, pre_gain).astype(BF16)
    low, high = jnp.split(jnp.concatenate([edge, normed], axis=0), 2, axis=1)
    spread = jnp.dot(jnp.where(core == 0, low, high), mine, preferred_element_type=F32)
    spread += jnp.dot(jnp.where(core == 0, high, low), other, preferred_element_type=F32)
    outer_part, inner_part, signal = jnp.split(spread, 3, axis=1)
    product = (inner_part * signal).astype(BF16).astype(F32)
    convolved = sum(
        product[lead - (TAPS - 1) + k : lead - (TAPS - 1) + k + rows] * conv_taps[k]
        for k in range(TAPS)
    )
    conv_mixed = (outer_part[lead:] * convolved).astype(BF16)
    conv_projected = jnp.dot(conv_mixed, conv_output, preferred_element_type=F32)

    groups = parts.shape[0]
    logs = parts[:, 128:].reshape(groups, 2, 8, 128)[:, :, :3].astype(F32)
    logs = logs[:, :, 0] + (logs[:, :, 1] + logs[:, :, 2])
    top = jnp.max(logs, axis=0)
    share = jnp.exp(logs - top)
    share_sum = jnp.sum(share, axis=0)
    row_logsum = top + jnp.log(share_sum)
    share = share / share_sum
    mixed_parts = parts[:, :128].reshape(groups, 2, VDIM, 128).astype(F32)
    heads = jnp.sum(mixed_parts * share[:, :, None, :], axis=0).astype(BF16).reshape(-1, rows)
    heads_projected = lax.dot_general(
        heads, heads_output, (((0,), (0,)), ((), ())), preferred_element_type=F32
    )
    projected = (conv_projected + heads_projected).astype(BF16)
    tp = lax.axis_size("tp")
    arrived = exchange(projected.reshape(tp, rows // tp, -1), "tp")
    projected = arrived.astype(F32).sum(axis=0)
    mixed = rms_scale(projected, post_gain).astype(BF16)
    return (mixed, row_logsum)


def solution(mesh):
    split = Mesh(mesh.devices.reshape(8, 2, 4, 2, mesh.shape["tp"]), SP_TP)
    return jax.shard_map(
        layer,
        mesh=split,
        in_specs=(
            P(SP, None),
            P(),
            P(SP, "tp"),
            P(SP, "tp"),
            P(SP, "tp"),
            P(None, "tp"),
            P(None, "tp"),
            P(None, "tp"),
            P(),
            P(),
            P(),
            P(None, "tp"),
            P(None, "tp"),
            P(None, "tp"),
            P(None, "tp"),
            P("tp", None),
            P("tp", None),
            P(),
        ),
        out_specs=(P(SP_TP, None), P("tp", SP)),
        check_vma=False,
    )
```

```python
import math

import jax
import jax.numpy as jnp
from jax import lax
from jax.experimental import pallas as pl
from jax.experimental.pallas import tpu as pltpu
from jax.sharding import Mesh
from jax.sharding import PartitionSpec as P

NOPE = 64
ROPE = 32
VDIM = 64
TAPS = 3
SP = ("far", "pair", "x", "core")
SP_TP = ("far", "pair", "x", "core", "tp")
Z = ("far", "pair")
GROUP = ("pair", "x", "core")

eps = 1e-06
rope_theta = 500000.0
SCALE = (NOPE + ROPE) ** (-0.5)
LOG2E = math.log2(math.e)
LOW = -1e30
BF16 = jnp.bfloat16
F32 = jnp.float32


def weight_rows(joint, depth, wide, cores):
    rows = joint[:, 2 * QUERY_ROWS :].reshape(wide, cores, -1, 6, depth, 128)
    rows = rows.transpose(2, 0, 1, 4, 3, 5)
    return rows.reshape(-1, 6 * 128)


def exchange(array, axis):
    return lax.all_to_all(array, axis, split_axis=0, concat_axis=0, tiled=True)


def shifted(value, axis, steps):
    count = lax.axis_size(axis)
    first, last = (max(0, -steps), min(count, count - steps))
    return lax.ppermute(value, axis, [(source, source + steps) for source in range(first, last)])


def rms_scale(values, scale_row):
    widened = values.astype(F32)
    return (
        widened * lax.rsqrt(jnp.mean(widened * widened, axis=-1, keepdims=True) + eps) * scale_row
    )


def dot_t(values, weights):
    return lax.dot_general(weights, values, (((0,), (1,)), ((), ())), preferred_element_type=F32)


def rotate_rows(values, cosine, sine):
    half = values.shape[-2] // 2
    leading = values[..., :half, :]
    trailing = values[..., half:, :]
    return jnp.concatenate(
        [leading * cosine - trailing * sine, trailing * cosine + leading * sine], axis=-2
    )


COLS = 256
QUERY_ROWS = 192
PART_ROWS = 144
FLOOR = -1e29


def attention_kernel(held_ref, query_ref, out_ref, key_rows, value_cols, query_full):
    far, here = lax.axis_index("far"), lax.axis_index(GROUP)
    blocks = held_ref.shape[0]
    near = query_ref.shape[0]
    groups = 2 * near
    queries = groups * 128
    for b in range(blocks):
        key_rows[b * 128 : (b + 1) * 128, :] = held_ref[b, 0:160, :].T
        value_cols[:, b * 128 : (b + 1) * 128] = held_ref[b, 160:288, :]
    for h in range(2):
        for g in range(groups):
            at = slice(h * queries + g * 128, h * queries + (g + 1) * 128)
            first = g // near * QUERY_ROWS
            query_full[h * 64 : (h + 1) * 64, at] = query_ref[
                g % near, first + h * 64 : first + (h + 1) * 64, :
            ]
            query_full[(1 - h) * 64 : (2 - h) * 64, at] = jnp.zeros((64, 128), BF16)
            query_full[128:160, at] = query_ref[
                g % near, first + 128 + h * 32 : first + 160 + h * 32, :
            ]
    factor = SCALE * LOG2E
    row = lax.broadcasted_iota(jnp.int32, (blocks * 128, 1), 0)
    key_at = row // 128 * queries + here * 128 + row % 128 - far * queries

    def score(first):
        return jnp.dot(
            key_rows[...], query_full[:, first : first + COLS], preferred_element_type=F32
        )

    def soften(first, scores):
        col = lax.broadcasted_iota(jnp.int32, (1, COLS), 1) + first % queries
        scores = jnp.where(key_at <= col, scores, LOW)
        best = jnp.maximum(jnp.max(scores, axis=0, keepdims=True), FLOOR)
        weights = jnp.exp2(scores * factor - best * factor)
        total = jnp.maximum(jnp.sum(weights, axis=0, keepdims=True), 1e-30)
        return weights.astype(BF16), total, best * SCALE + jnp.log(total)

    logs = {}

    def mix(first, weights, total, logsum):
        h = first // queries
        mixed = jnp.dot(
            value_cols[h * 64 : (h + 1) * 64, :], weights, preferred_element_type=F32
        )
        mixed = (mixed * (1.0 / total)).astype(BF16)
        high = logsum.astype(BF16).astype(F32)
        middle = (logsum - high).astype(BF16).astype(F32)
        low = logsum - high - middle
        tail = jnp.concatenate([high, middle, low, jnp.zeros((5, COLS), F32)], axis=0)
        for i in range(COLS // 128):
            g = first % queries // 128 + i
            at = slice(i * 128, (i + 1) * 128)
            out_ref[g, h * 64 : (h + 1) * 64, :] = mixed[:, at]
            if h == 0:
                logs[g] = tail[:, at]
            else:
                both = jnp.concatenate([logs.pop(g), tail[:, at]], axis=0)
                out_ref[g, 128:PART_ROWS, :] = both.astype(BF16)

    tiles = 2 * queries // COLS
    scores, softened = {}, {}
    for n in range(tiles + 2):
        if 0 <= n - 1 < tiles:
            softened[n - 1] = soften((n - 1) * COLS, scores.pop(n - 1))
        if n < tiles:
            scores[n] = score(n * COLS)
        if 0 <= n - 2 < tiles:
            mix((n - 2) * COLS, *softened.pop(n - 2))


def attend(held, joint):
    blocks, groups = held.shape[0], 2 * joint.shape[0]
    width = 2 * groups * 128
    return pl.pallas_call(
        attention_kernel,
        out_shape=jax.ShapeDtypeStruct((groups, PART_ROWS, 128), BF16),
        grid=(1,),
        in_specs=[
            pl.BlockSpec(held.shape, lambda i: (0, 0, 0)),
            pl.BlockSpec((groups // 2, 2 * QUERY_ROWS, 128), lambda i: (0, 0, 0)),
        ],
        out_specs=pl.BlockSpec((groups, PART_ROWS, 128), lambda i: (0, 0, 0)),
        scratch_shapes=[
            pltpu.VMEM((blocks * 128, 160), BF16),
            pltpu.VMEM((128, blocks * 128), BF16),
            pltpu.VMEM((160, width), BF16),
        ],
        cost_estimate=pl.CostEstimate(
            flops=2 * blocks * 128 * width * (160 + 64),
            bytes_accessed=2_000_000,
            transcendentals=blocks * 128 * width,
        ),
        name="attend",
    )(held, joint)


def dot_nt(left, right):
    return lax.dot_general(left, right, (((1,), (1,)), ((), ())), preferred_element_type=F32)


def gates_kernel(outer_ref, inner_ref, signal_ref, out_ref):
    depth = outer_ref.shape[0]
    at = 0
    for ref in (outer_ref, inner_ref, signal_ref):
        for first in range(0, ref.shape[1], 128):
            block = ref[:, first : first + 128]
            for d in range(out_ref.shape[0]):
                out_ref[d, at : at + depth, :] = block
            at += depth


def spread_gates(gates, copies):
    depth, width = gates[0].shape
    return pl.pallas_call(
        gates_kernel,
        out_shape=jax.ShapeDtypeStruct((copies, 3 * depth * width // 128, 128), BF16),
        cost_estimate=pl.CostEstimate(flops=1_000_000, bytes_accessed=400_000, transcendentals=0),
        name="spread_gates",
    )(*gates)


def entry_kernel(tokens, gain, latent_down, query_down, rotary_down, normed_ref, latent_ref, rot_ref):
    wide = tokens[...].astype(F32)
    scale = lax.rsqrt(jnp.mean(wide * wide, axis=-1, keepdims=True) + eps)
    normed = (wide * scale * gain[...]).astype(BF16)
    normed_ref[...] = normed
    n = latent_down.shape[1]
    latent_ref[:, :n] = jnp.dot(
        normed, latent_down[...], preferred_element_type=F32
    ).astype(BF16)
    latent_ref[:, n:] = dot_nt(normed, query_down[...]).astype(BF16)
    rot_ref[...] = dot_nt(rotary_down[...], normed)


def entry(tokens, gain, latent_down, query_down, rotary_down):
    rows, width = tokens.shape
    columns = latent_down.shape[1] + query_down.shape[1]
    return pl.pallas_call(
        entry_kernel,
        out_shape=(
            jax.ShapeDtypeStruct((rows, width), BF16),
            jax.ShapeDtypeStruct((rows, columns), BF16),
            jax.ShapeDtypeStruct((ROPE, rows), F32),
        ),
        cost_estimate=pl.CostEstimate(
            flops=2 * rows * width * 384, bytes_accessed=2_500_000, transcendentals=rows
        ),
        name="entry",
    )(tokens, gain.reshape(1, -1), latent_down, query_down.T, rotary_down.T)


def merge_kernel(parts_ref, conv_ref, weight_ref, out_ref, logsum_ref):
    groups = parts_ref.shape[0]
    tails = parts_ref[:, 128:PART_ROWS, :].astype(F32)
    heads = []
    for h in range(2):
        logs = tails[:, 8 * h, :] + (tails[:, 8 * h + 1, :] + tails[:, 8 * h + 2, :])
        top = jnp.max(logs, axis=0, keepdims=True)
        share = jnp.exp(logs - top)
        share_sum = jnp.sum(share, axis=0, keepdims=True)
        logsum_ref[h : h + 1, :] = top + jnp.log(share_sum)
        share = share / share_sum
        mixed = jnp.zeros((VDIM, 128), F32)
        for g in range(groups):
            part = parts_ref[g, h * VDIM : (h + 1) * VDIM, :].astype(F32)
            mixed = mixed + part * share[g : g + 1, :]
        heads.append(mixed)
    mixed = jnp.concatenate(heads, axis=0).T.astype(BF16)
    for first in range(0, out_ref.shape[1], 512):
        at = slice(first, first + 512)
        out_ref[:, at] = (
            conv_ref[:, at]
            + jnp.dot(mixed, weight_ref[:, at], preferred_element_type=F32)
        ).astype(BF16)


def merge(parts, conv_projected, heads_output):
    rows, width = conv_projected.shape
    return pl.pallas_call(
        merge_kernel,
        out_shape=(
            jax.ShapeDtypeStruct((rows, width), BF16),
            jax.ShapeDtypeStruct((2, rows), F32),
        ),
        cost_estimate=pl.CostEstimate(
            flops=2 * rows * width * 128, bytes_accessed=2_000_000, transcendentals=rows * 32
        ),
        name="merge",
    )(parts, conv_projected, heads_output)


def layer(
    tokens,
    pre_gain,
    outer_gate,
    inner_gate,
    conv_input,
    conv_taps,
    query_down,
    latent_down,
    rotary_down,
    query_gain,
    latent_gain,
    query_up,
    query_rotary,
    key_up,
    value_up,
    conv_output,
    heads_output,
    post_gain,
):
    rows = tokens.shape[0]
    sp_index = lax.axis_index(SP)
    core = lax.axis_index("core")

    depth = outer_gate.shape[0]
    gates = spread_gates((outer_gate, inner_gate, conv_input), lax.axis_size(Z))
    gates = exchange(gates, Z)

    edge = shifted(tokens[rows - (TAPS - 1) :], SP, 1)

    normed, latents, key_raw = entry(tokens, pre_gain, latent_down, query_down, rotary_down)
    latents = lax.all_gather(latents, "tp", axis=0)

    positions = sp_index * rows + jnp.arange(rows, dtype=jnp.int32)
    frequency = rope_theta ** (-jnp.arange(ROPE // 2, dtype=F32) / (ROPE // 2))
    angles = positions.astype(F32)[None, :] * frequency[:, None]
    cosine, sine = jnp.cos(angles), jnp.sin(angles)
    key_turned = rotate_rows(key_raw, cosine, sine).astype(BF16)

    n_latent = latent_down.shape[1]
    key_latent = jnp.moveaxis(latents[:, :, :n_latent], 0, 1).reshape(rows, -1)
    query_latent = jnp.moveaxis(latents[:, :, n_latent:], 0, 1).reshape(rows, -1)
    latent_normed = rms_scale(key_latent, latent_gain).astype(BF16)
    query_normed = rms_scale(query_latent, query_gain).astype(BF16)
    query_nope = dot_t(query_normed, query_up).astype(BF16)
    turned = dot_t(query_normed, query_rotary).reshape(-1, ROPE, rows)
    turned = rotate_rows(turned, cosine, sine).astype(BF16).reshape(-1, rows)
    queries = jnp.concatenate([query_nope, turned], axis=0)
    queries_other = lax.ppermute(queries, "pair", [(0, 1), (1, 0)])
    first_of_pair = lax.axis_index("pair") == 0
    both = [
        jnp.where(first_of_pair, queries, queries_other),
        jnp.where(first_of_pair, queries_other, queries),
    ]
    _, wide, cores = (lax.axis_size(name) for name in GROUP)
    halves = gates.reshape(cores, -1, 128)
    both = jnp.broadcast_to(jnp.concatenate(both, axis=0), (wide, cores, 2 * QUERY_ROWS, 128))
    halves = jnp.broadcast_to(halves, (wide, *halves.shape))
    sent = jnp.concatenate([both, halves], axis=2)
    joint = exchange(sent.reshape(-1, *sent.shape[2:]), GROUP[1:])
    joint_other = lax.ppermute(joint, "core", [(0, 1), (1, 0)])
    held = jnp.concatenate(
        [
            dot_t(latent_normed, key_up).astype(BF16),
            key_turned,
            dot_t(latent_normed, value_up).astype(BF16),
        ],
        axis=0,
    )
    held = lax.all_gather(held, "far", axis=0, tiled=True).reshape(-1, *held.shape)

    parts = attend(held, joint)
    parts = exchange(parts, GROUP)

    mine, other = (weight_rows(whole, depth, wide, cores) for whole in (joint, joint_other))
    lead = 16
    edge = jnp.pad(edge, ((lead - (TAPS - 1), 0), (0, 0)))
    edge = rms_scale(edge, pre_gain).astype(BF16)
    low, high = jnp.split(jnp.concatenate([edge, normed], axis=0), 2, axis=1)
    spread = jnp.dot(jnp.where(core == 0, low, high), mine, preferred_element_type=F32)
    spread += jnp.dot(jnp.where(core == 0, high, low), other, preferred_element_type=F32)
    outer_part, inner_part, signal = jnp.split(spread, 3, axis=1)
    product = (inner_part * signal).astype(BF16).astype(F32)
    convolved = sum(
        product[lead - (TAPS - 1) + k : lead - (TAPS - 1) + k + rows] * conv_taps[k]
        for k in range(TAPS)
    )
    conv_mixed = (outer_part[lead:] * convolved).astype(BF16)
    conv_projected = jnp.dot(conv_mixed, conv_output, preferred_element_type=F32)

    projected, row_logsum = merge(parts, conv_projected, heads_output)
    tp = lax.axis_size("tp")
    arrived = exchange(projected.reshape(tp, rows // tp, -1), "tp")
    projected = arrived.astype(F32).sum(axis=0)
    mixed = rms_scale(projected, post_gain).astype(BF16)
    return (mixed, row_logsum)


def solution(mesh):
    split = Mesh(mesh.devices.reshape(8, 2, 4, 2, mesh.shape["tp"]), SP_TP)
    return jax.shard_map(
        layer,
        mesh=split,
        in_specs=(
            P(SP, None),
            P(),
            P(SP, "tp"),
            P(SP, "tp"),
            P(SP, "tp"),
            P(None, "tp"),
            P(None, "tp"),
            P(None, "tp"),
            P(),
            P(),
            P(),
            P(None, "tp"),
            P(None, "tp"),
            P(None, "tp"),
            P(None, "tp"),
            P("tp", None),
            P("tp", None),
            P(),
        ),
        out_specs=(P(SP_TP, None), P("tp", SP)),
        check_vma=False,
    )
```

```python
import math

import jax
import jax.numpy as jnp
from jax import lax
from jax.experimental import pallas as pl
from jax.experimental.pallas import tpu as pltpu
from jax.sharding import Mesh
from jax.sharding import PartitionSpec as P

NOPE = 64
ROPE = 32
VDIM = 64
TAPS = 3
SP = ("far", "pair", "x", "core")
SP_TP = ("far", "pair", "x", "core", "tp")
Z = ("far", "pair")
GROUP = ("pair", "x", "core")

eps = 1e-06
rope_theta = 500000.0
SCALE = (NOPE + ROPE) ** (-0.5)
LOG2E = math.log2(math.e)
LOW = -1e30
BF16 = jnp.bfloat16
F32 = jnp.float32


def exchange(array, axis):
    return lax.all_to_all(array, axis, split_axis=0, concat_axis=0, tiled=True)


def shifted(value, axis, steps):
    count = lax.axis_size(axis)
    first, last = (max(0, -steps), min(count, count - steps))
    return lax.ppermute(value, axis, [(source, source + steps) for source in range(first, last)])


def rms_scale(values, scale_row):
    widened = values.astype(F32)
    return (
        widened * lax.rsqrt(jnp.mean(widened * widened, axis=-1, keepdims=True) + eps) * scale_row
    )


def dot_t(values, weights):
    return lax.dot_general(weights, values, (((0,), (1,)), ((), ())), preferred_element_type=F32)


def rotate_rows(values, cosine, sine):
    half = values.shape[-2] // 2
    leading = values[..., :half, :]
    trailing = values[..., half:, :]
    return jnp.concatenate(
        [leading * cosine - trailing * sine, trailing * cosine + leading * sine], axis=-2
    )


COLS = 256
QUERY_ROWS = 192
PART_ROWS = 144
FLOOR = -1e29


def attention_kernel(held_ref, query_ref, out_ref, key_rows, value_cols, query_full):
    far, here = lax.axis_index("far"), lax.axis_index(GROUP)
    blocks = held_ref.shape[0]
    near = query_ref.shape[0]
    groups = 2 * near
    queries = groups * 128
    for b in range(blocks):
        key_rows[b * 128 : (b + 1) * 128, :] = held_ref[b, 0:160, :].T
        value_cols[:, b * 128 : (b + 1) * 128] = held_ref[b, 160:288, :]
    for h in range(2):
        for g in range(groups):
            at = slice(h * queries + g * 128, h * queries + (g + 1) * 128)
            first = g // near * QUERY_ROWS
            query_full[h * 64 : (h + 1) * 64, at] = query_ref[
                g % near, first + h * 64 : first + (h + 1) * 64, :
            ]
            query_full[(1 - h) * 64 : (2 - h) * 64, at] = jnp.zeros((64, 128), BF16)
            query_full[128:160, at] = query_ref[
                g % near, first + 128 + h * 32 : first + 160 + h * 32, :
            ]
    factor = SCALE * LOG2E
    row = lax.broadcasted_iota(jnp.int32, (blocks * 128, 1), 0)
    key_at = row // 128 * queries + here * 128 + row % 128 - far * queries

    def score(first):
        return jnp.dot(
            key_rows[...], query_full[:, first : first + COLS], preferred_element_type=F32
        )

    def soften(first, scores):
        col = lax.broadcasted_iota(jnp.int32, (1, COLS), 1) + first % queries
        scores = jnp.where(key_at <= col, scores, LOW)
        best = jnp.maximum(jnp.max(scores, axis=0, keepdims=True), FLOOR)
        weights = jnp.exp2(scores * factor - best * factor)
        total = jnp.maximum(jnp.sum(weights, axis=0, keepdims=True), 1e-30)
        return weights.astype(BF16), total, best * SCALE + jnp.log(total)

    logs = {}

    def mix(first, weights, total, logsum):
        h = first // queries
        mixed = jnp.dot(
            value_cols[h * 64 : (h + 1) * 64, :], weights, preferred_element_type=F32
        )
        mixed = (mixed * (1.0 / total)).astype(BF16)
        high = logsum.astype(BF16).astype(F32)
        middle = (logsum - high).astype(BF16).astype(F32)
        low = logsum - high - middle
        tail = jnp.concatenate([high, middle, low, jnp.zeros((5, COLS), F32)], axis=0)
        for i in range(COLS // 128):
            g = first % queries // 128 + i
            at = slice(i * 128, (i + 1) * 128)
            out_ref[g, h * 64 : (h + 1) * 64, :] = mixed[:, at]
            if h == 0:
                logs[g] = tail[:, at]
            else:
                both = jnp.concatenate([logs.pop(g), tail[:, at]], axis=0)
                out_ref[g, 128:PART_ROWS, :] = both.astype(BF16)

    tiles = 2 * queries // COLS
    scores, softened = {}, {}
    for n in range(tiles + 2):
        if 0 <= n - 1 < tiles:
            softened[n - 1] = soften((n - 1) * COLS, scores.pop(n - 1))
        if n < tiles:
            scores[n] = score(n * COLS)
        if 0 <= n - 2 < tiles:
            mix((n - 2) * COLS, *softened.pop(n - 2))


def attend(held, joint):
    blocks, groups = held.shape[0], 2 * joint.shape[0]
    width = 2 * groups * 128
    return pl.pallas_call(
        attention_kernel,
        out_shape=jax.ShapeDtypeStruct((groups, PART_ROWS, 128), BF16),
        grid=(1,),
        in_specs=[
            pl.BlockSpec(held.shape, lambda i: (0, 0, 0)),
            pl.BlockSpec((groups // 2, 2 * QUERY_ROWS, 128), lambda i: (0, 2, 0)),
        ],
        out_specs=pl.BlockSpec((groups, PART_ROWS, 128), lambda i: (0, 0, 0)),
        scratch_shapes=[
            pltpu.VMEM((blocks * 128, 160), BF16),
            pltpu.VMEM((128, blocks * 128), BF16),
            pltpu.VMEM((160, width), BF16),
        ],
        compiler_params=pltpu.CompilerParams(vmem_limit_bytes=56 << 20),
        cost_estimate=pl.CostEstimate(
            flops=2 * blocks * 128 * width * (160 + 64),
            bytes_accessed=2_000_000,
            transcendentals=blocks * 128 * width,
        ),
        name="attend",
    )(held, joint)


def dot_nt(left, right):
    return lax.dot_general(left, right, (((1,), (1,)), ((), ())), preferred_element_type=F32)


def gates_kernel(outer_ref, inner_ref, signal_ref, out_ref):
    depth = outer_ref.shape[0]
    at = 0
    for ref in (outer_ref, inner_ref, signal_ref):
        for first in range(0, ref.shape[1], 128):
            block = ref[:, first : first + 128]
            for d in range(out_ref.shape[0]):
                out_ref[d, at : at + depth, :] = block
            at += depth


def spread_gates(gates, copies):
    depth, width = gates[0].shape
    return pl.pallas_call(
        gates_kernel,
        out_shape=jax.ShapeDtypeStruct((copies, 3 * depth * width // 128, 128), BF16),
        cost_estimate=pl.CostEstimate(flops=1_000_000, bytes_accessed=400_000, transcendentals=0),
        name="spread_gates",
    )(*gates)


def entry_kernel(tokens, gain, latent_down, query_down, rotary_down, normed_ref, latent_ref, rot_ref):
    wide = tokens[...].astype(F32)
    scale = lax.rsqrt(jnp.mean(wide * wide, axis=-1, keepdims=True) + eps)
    normed = (wide * scale * gain[...]).astype(BF16)
    normed_ref[...] = normed
    n = latent_down.shape[1]
    latent_ref[:, :n] = jnp.dot(
        normed, latent_down[...], preferred_element_type=F32
    ).astype(BF16)
    latent_ref[:, n:] = dot_nt(normed, query_down[...]).astype(BF16)
    rot_ref[...] = dot_nt(rotary_down[...], normed)


def entry(tokens, gain, latent_down, query_down, rotary_down):
    rows, width = tokens.shape
    columns = latent_down.shape[1] + query_down.shape[1]
    return pl.pallas_call(
        entry_kernel,
        out_shape=(
            jax.ShapeDtypeStruct((rows, width), BF16),
            jax.ShapeDtypeStruct((rows, columns), BF16),
            jax.ShapeDtypeStruct((ROPE, rows), F32),
        ),
        cost_estimate=pl.CostEstimate(
            flops=2 * rows * width * 384, bytes_accessed=2_500_000, transcendentals=rows
        ),
        name="entry",
    )(tokens, gain.reshape(1, -1), latent_down, query_down.T, rotary_down.T)


LEAD = 16


def conv_kernel(
    mine_ref, other_ref, normed_ref, edge_ref, gain_ref, taps_ref, output_ref, out_ref,
    rows_ref, weight_ref, product_ref,
):
    core = lax.axis_index("core")
    near, _, _ = mine_ref.shape
    count, width = normed_ref.shape
    half = width // 2
    wide = edge_ref[...].astype(F32)
    scale = lax.rsqrt(jnp.mean(wide * wide, axis=-1, keepdims=True) + eps)
    rows_ref[:LEAD, :] = (wide * scale * gain_ref[...]).astype(BF16)
    rows_ref[LEAD:, :] = normed_ref[...]
    columns = weight_ref.shape[1]
    depth = 128 // near
    for side, ref in enumerate((mine_ref, other_ref)):
        for block in range(half // 128):
            for source in range(near):
                to = side * half + block * 128 + source * depth
                for b in range(columns // 128):
                    at = (block * (columns // 128) + b) * depth
                    weight_ref[to : to + depth, b * 128 : (b + 1) * 128] = ref[
                        source, at : at + depth, :
                    ]
    own = pl.ds(pl.multiple_of(core * half, half), half)
    rest = pl.ds(pl.multiple_of((1 - core) * half, half), half)
    spread = jnp.dot(rows_ref[:, own], weight_ref[:half, :], preferred_element_type=F32)
    spread += jnp.dot(rows_ref[:, rest], weight_ref[half:, :], preferred_element_type=F32)
    third = columns // 3
    product = spread[:, third : 2 * third] * spread[:, 2 * third :]
    product_ref[...] = product.astype(BF16).astype(F32)
    convolved = jnp.zeros((count, third), F32)
    for k in range(TAPS):
        first = LEAD - (TAPS - 1) + k
        convolved = convolved + product_ref[first : first + count, :] * taps_ref[k : k + 1, :]
    mixed = (spread[LEAD:, :third] * convolved).astype(BF16)
    for first in range(0, out_ref.shape[1], 512):
        at = slice(first, first + 512)
        out_ref[:, at] = jnp.dot(mixed, output_ref[:, at], preferred_element_type=F32)


def convolve(joint, joint_other, normed, edge, gain, taps, output):
    count, width = normed.shape
    third, out_width = output.shape
    near = joint.shape[0]
    weights = pl.BlockSpec((near, joint.shape[1] - 2 * QUERY_ROWS, 128), lambda i: (0, 0, 0))
    whole = [pl.BlockSpec(a.shape, lambda i: (0, 0)) for a in (normed, edge, gain, taps, output)]
    return pl.pallas_call(
        conv_kernel,
        out_shape=jax.ShapeDtypeStruct((count, out_width), F32),
        grid=(1,),
        in_specs=[weights, weights, *whole],
        out_specs=pl.BlockSpec((count, out_width), lambda i: (0, 0)),
        scratch_shapes=[
            pltpu.VMEM((LEAD + count, width), BF16),
            pltpu.VMEM((width, 3 * third), BF16),
            pltpu.VMEM((LEAD + count, third), F32),
        ],
        cost_estimate=pl.CostEstimate(
            flops=2 * count * (width * 3 * third + third * out_width),
            bytes_accessed=6_000_000,
            transcendentals=0,
        ),
        compiler_params=pltpu.CompilerParams(vmem_limit_bytes=30 << 20),
        name="convolve",
    )(joint, joint_other, normed, edge, gain, taps, output)


def merge_kernel(parts_ref, conv_ref, weight_ref, out_ref, top_ref, log_ref):
    groups = parts_ref.shape[0]
    tails = parts_ref[:, 128:PART_ROWS, :].astype(F32)
    heads = []
    for h in range(2):
        logs = tails[:, 8 * h, :] + (tails[:, 8 * h + 1, :] + tails[:, 8 * h + 2, :])
        top = jnp.max(logs, axis=0, keepdims=True)
        share = jnp.exp(logs - top)
        share_sum = jnp.sum(share, axis=0, keepdims=True)
        top_ref[h : h + 1, :] = top
        log_ref[h : h + 1, :] = jnp.log(share_sum)
        share = share / share_sum
        mixed = jnp.zeros((VDIM, 128), F32)
        for g in range(groups):
            part = parts_ref[g, h * VDIM : (h + 1) * VDIM, :].astype(F32)
            mixed = mixed + part * share[g : g + 1, :]
        heads.append(mixed)
    mixed = jnp.concatenate(heads, axis=0).T.astype(BF16)
    for first in range(0, out_ref.shape[1], 512):
        at = slice(first, first + 512)
        out_ref[:, at] = (
            conv_ref[:, at]
            + jnp.dot(mixed, weight_ref[:, at], preferred_element_type=F32)
        ).astype(BF16)


def merge(parts, conv_projected, heads_output):
    rows, width = conv_projected.shape
    return pl.pallas_call(
        merge_kernel,
        out_shape=(
            jax.ShapeDtypeStruct((rows, width), BF16),
            jax.ShapeDtypeStruct((2, rows), F32),
            jax.ShapeDtypeStruct((2, rows), F32),
        ),
        cost_estimate=pl.CostEstimate(
            flops=2 * rows * width * 128, bytes_accessed=2_000_000, transcendentals=rows * 32
        ),
        compiler_params=pltpu.CompilerParams(vmem_limit_bytes=16 << 20),
        name="merge",
    )(parts, conv_projected, heads_output)


def layer(
    tokens,
    pre_gain,
    outer_gate,
    inner_gate,
    conv_input,
    conv_taps,
    query_down,
    latent_down,
    rotary_down,
    query_gain,
    latent_gain,
    query_up,
    query_rotary,
    key_up,
    value_up,
    conv_output,
    heads_output,
    post_gain,
):
    rows = tokens.shape[0]
    sp_index = lax.axis_index(SP)

    gates = spread_gates((outer_gate, inner_gate, conv_input), lax.axis_size(Z))
    gates = exchange(gates, Z)

    edge = shifted(tokens[rows - LEAD :], SP, 1)

    normed, latents, key_raw = entry(tokens, pre_gain, latent_down, query_down, rotary_down)
    latents = lax.all_gather(latents, "tp", axis=0)

    positions = sp_index * rows + jnp.arange(rows, dtype=jnp.int32)
    frequency = rope_theta ** (-jnp.arange(ROPE // 2, dtype=F32) / (ROPE // 2))
    angles = positions.astype(F32)[None, :] * frequency[:, None]
    cosine, sine = jnp.cos(angles), jnp.sin(angles)
    key_turned = rotate_rows(key_raw, cosine, sine).astype(BF16)

    n_latent = latent_down.shape[1]
    key_latent = jnp.moveaxis(latents[:, :, :n_latent], 0, 1).reshape(rows, -1)
    query_latent = jnp.moveaxis(latents[:, :, n_latent:], 0, 1).reshape(rows, -1)
    latent_normed = rms_scale(key_latent, latent_gain).astype(BF16)
    query_normed = rms_scale(query_latent, query_gain).astype(BF16)
    query_nope = dot_t(query_normed, query_up).astype(BF16)
    turned = dot_t(query_normed, query_rotary).reshape(-1, ROPE, rows)
    turned = rotate_rows(turned, cosine, sine).astype(BF16).reshape(-1, rows)
    queries = jnp.concatenate([query_nope, turned], axis=0)
    queries_other = lax.ppermute(queries, "pair", [(0, 1), (1, 0)])
    first_of_pair = lax.axis_index("pair") == 0
    both = [
        jnp.where(first_of_pair, queries, queries_other),
        jnp.where(first_of_pair, queries_other, queries),
    ]
    _, wide, cores = (lax.axis_size(name) for name in GROUP)
    halves = gates.reshape(cores, -1, 128)
    both = jnp.broadcast_to(jnp.concatenate(both, axis=0), (wide, cores, 2 * QUERY_ROWS, 128))
    halves = jnp.broadcast_to(halves, (wide, *halves.shape))
    sent = jnp.concatenate([halves, both], axis=2)
    joint = exchange(sent.reshape(-1, *sent.shape[2:]), GROUP[1:])
    joint_other = lax.ppermute(joint, "core", [(0, 1), (1, 0)])
    held = jnp.concatenate(
        [
            dot_t(latent_normed, key_up).astype(BF16),
            key_turned,
            dot_t(latent_normed, value_up).astype(BF16),
        ],
        axis=0,
    )
    held = lax.all_gather(held, "far", axis=0, tiled=True).reshape(-1, *held.shape)

    parts = attend(held, joint)
    parts = exchange(parts, GROUP)

    conv_projected = convolve(
        joint,
        joint_other,
        normed,
        edge,
        pre_gain.reshape(1, -1),
        conv_taps,
        conv_output,
    )
    projected, top, log_total = merge(parts, conv_projected, heads_output)
    tp = lax.axis_size("tp")
    arrived = exchange(projected.reshape(tp, rows // tp, -1), "tp")
    row_logsum = top + log_total
    projected = arrived.astype(F32).sum(axis=0)
    mixed = rms_scale(projected, post_gain).astype(BF16)
    return (mixed, row_logsum)


def solution(mesh):
    split = Mesh(mesh.devices.reshape(8, 2, 4, 2, mesh.shape["tp"]), SP_TP)
    return jax.shard_map(
        layer,
        mesh=split,
        in_specs=(
            P(SP, None),
            P(),
            P(SP, "tp"),
            P(SP, "tp"),
            P(SP, "tp"),
            P(None, "tp"),
            P(None, "tp"),
            P(None, "tp"),
            P(),
            P(),
            P(),
            P(None, "tp"),
            P(None, "tp"),
            P(None, "tp"),
            P(None, "tp"),
            P("tp", None),
            P("tp", None),
            P(),
        ),
        out_specs=(P(SP_TP, None), P("tp", SP)),
        check_vma=False,
    )
```

```python
import math

import jax
import jax.numpy as jnp
from jax import lax
from jax.experimental import pallas as pl
from jax.experimental.pallas import tpu as pltpu
from jax.sharding import Mesh
from jax.sharding import PartitionSpec as P

NOPE = 64
ROPE = 32
VDIM = 64
TAPS = 3
SP = ("far", "pair", "x", "core")
SP_TP = ("far", "pair", "x", "core", "tp")
Z = ("far", "pair")
GROUP = ("pair", "x", "core")

eps = 1e-06
rope_theta = 500000.0
SCALE = (NOPE + ROPE) ** (-0.5)
LOG2E = math.log2(math.e)
LOW = -1e30
BF16 = jnp.bfloat16
F32 = jnp.float32


def exchange(array, axis):
    return lax.all_to_all(array, axis, split_axis=0, concat_axis=0, tiled=True)


def shifted(value, axis, steps):
    count = lax.axis_size(axis)
    first, last = (max(0, -steps), min(count, count - steps))
    return lax.ppermute(value, axis, [(source, source + steps) for source in range(first, last)])


def rms_scale(values, scale_row):
    widened = values.astype(F32)
    return (
        widened * lax.rsqrt(jnp.mean(widened * widened, axis=-1, keepdims=True) + eps) * scale_row
    )


def dot_t(values, weights):
    return lax.dot_general(weights, values, (((0,), (1,)), ((), ())), preferred_element_type=F32)


def rotate_rows(values, cosine, sine):
    half = values.shape[-2] // 2
    leading = values[..., :half, :]
    trailing = values[..., half:, :]
    return jnp.concatenate(
        [leading * cosine - trailing * sine, trailing * cosine + leading * sine], axis=-2
    )


COLS = 256
QUERY_ROWS = 192
PART_ROWS = 144
FLOOR = -1e29


def attention_kernel(held_ref, query_ref, out_ref, key_rows, value_cols, query_full):
    far, here = lax.axis_index("far"), lax.axis_index(GROUP)
    blocks = held_ref.shape[0]
    near = query_ref.shape[0]
    groups = 2 * near
    queries = groups * 128
    for b in range(blocks):
        key_rows[b * 128 : (b + 1) * 128, :] = held_ref[b, 0:160, :].T
        value_cols[:, b * 128 : (b + 1) * 128] = held_ref[b, 160:288, :]
    for h in range(2):
        for g in range(groups):
            at = slice(h * queries + g * 128, h * queries + (g + 1) * 128)
            first = g // near * QUERY_ROWS
            query_full[h * 64 : (h + 1) * 64, at] = query_ref[
                g % near, first + h * 64 : first + (h + 1) * 64, :
            ]
            query_full[(1 - h) * 64 : (2 - h) * 64, at] = jnp.zeros((64, 128), BF16)
            query_full[128:160, at] = query_ref[
                g % near, first + 128 + h * 32 : first + 160 + h * 32, :
            ]
    factor = SCALE * LOG2E
    row = lax.broadcasted_iota(jnp.int32, (blocks * 128, 1), 0)
    key_at = row // 128 * queries + here * 128 + row % 128 - far * queries

    def score(first):
        return jnp.dot(
            key_rows[...], query_full[:, first : first + COLS], preferred_element_type=F32
        )

    def soften(first, scores):
        col = lax.broadcasted_iota(jnp.int32, (1, COLS), 1) + first % queries
        scores = jnp.where(key_at <= col, scores, LOW)
        best = jnp.maximum(jnp.max(scores, axis=0, keepdims=True), FLOOR)
        weights = jnp.exp2(scores * factor - best * factor)
        total = jnp.maximum(jnp.sum(weights, axis=0, keepdims=True), 1e-30)
        return weights.astype(BF16), total, best * SCALE + jnp.log(total)

    logs = {}

    def mix(first, weights, total, logsum):
        h = first // queries
        mixed = jnp.dot(
            value_cols[h * 64 : (h + 1) * 64, :], weights, preferred_element_type=F32
        )
        mixed = (mixed * (1.0 / total)).astype(BF16)
        high = logsum.astype(BF16).astype(F32)
        middle = (logsum - high).astype(BF16).astype(F32)
        low = logsum - high - middle
        tail = jnp.concatenate([high, middle, low, jnp.zeros((5, COLS), F32)], axis=0)
        for i in range(COLS // 128):
            g = first % queries // 128 + i
            at = slice(i * 128, (i + 1) * 128)
            out_ref[g, h * 64 : (h + 1) * 64, :] = mixed[:, at]
            if h == 0:
                logs[g] = tail[:, at]
            else:
                both = jnp.concatenate([logs.pop(g), tail[:, at]], axis=0)
                out_ref[g, 128:PART_ROWS, :] = both.astype(BF16)

    tiles = 2 * queries // COLS
    scores, softened = {}, {}
    for n in range(tiles + 2):
        if 0 <= n - 1 < tiles:
            softened[n - 1] = soften((n - 1) * COLS, scores.pop(n - 1))
        if n < tiles:
            scores[n] = score(n * COLS)
        if 0 <= n - 2 < tiles:
            mix((n - 2) * COLS, *softened.pop(n - 2))


def attend(held, joint):
    blocks, groups = held.shape[0], 2 * joint.shape[0]
    width = 2 * groups * 128
    return pl.pallas_call(
        attention_kernel,
        out_shape=pltpu.HBM((groups, PART_ROWS, 128), BF16),
        grid=(1,),
        in_specs=[
            pl.BlockSpec(held.shape, lambda i: (0, 0, 0)),
            pl.BlockSpec((groups // 2, 2 * QUERY_ROWS, 128), lambda i: (0, 2, 0)),
        ],
        out_specs=pl.BlockSpec((groups, PART_ROWS, 128), lambda i: (0, 0, 0)),
        scratch_shapes=[
            pltpu.VMEM((blocks * 128, 160), BF16),
            pltpu.VMEM((128, blocks * 128), BF16),
            pltpu.VMEM((160, width), BF16),
        ],
        compiler_params=pltpu.CompilerParams(vmem_limit_bytes=48 << 20),
        cost_estimate=pl.CostEstimate(
            flops=2 * blocks * 128 * width * (160 + 64),
            bytes_accessed=2_000_000,
            transcendentals=blocks * 128 * width,
        ),
        name="attend",
    )(held, joint)


def dot_nt(left, right):
    return lax.dot_general(left, right, (((1,), (1,)), ((), ())), preferred_element_type=F32)


def gates_kernel(outer_ref, inner_ref, signal_ref, out_ref):
    depth = outer_ref.shape[0]
    at = 0
    for ref in (outer_ref, inner_ref, signal_ref):
        for first in range(0, ref.shape[1], 128):
            block = ref[:, first : first + 128]
            for d in range(out_ref.shape[0]):
                out_ref[d, at : at + depth, :] = block
            at += depth


def spread_gates(gates, copies):
    depth, width = gates[0].shape
    return pl.pallas_call(
        gates_kernel,
        out_shape=jax.ShapeDtypeStruct((copies, 3 * depth * width // 128, 128), BF16),
        cost_estimate=pl.CostEstimate(flops=1_000_000, bytes_accessed=400_000, transcendentals=0),
        name="spread_gates",
    )(*gates)


def entry_kernel(
    tokens, gain, latent_down, query_down, rotary_down, normed_ref, tail_ref, latent_ref, rot_ref
):
    wide = tokens[...].astype(F32)
    scale = lax.rsqrt(jnp.mean(wide * wide, axis=-1, keepdims=True) + eps)
    normed = (wide * scale * gain[...]).astype(BF16)
    normed_ref[...] = normed
    tail_ref[...] = normed[normed.shape[0] - LEAD :, :]
    n = latent_down.shape[1]
    latent_ref[:, :n] = jnp.dot(
        normed, latent_down[...], preferred_element_type=F32
    ).astype(BF16)
    latent_ref[:, n:] = dot_nt(normed, query_down[...]).astype(BF16)
    rot_ref[...] = dot_nt(rotary_down[...], normed)


def entry(tokens, gain, latent_down, query_down, rotary_down):
    rows, width = tokens.shape
    columns = latent_down.shape[1] + query_down.shape[1]
    return pl.pallas_call(
        entry_kernel,
        out_shape=(
            jax.ShapeDtypeStruct((rows, width), BF16),
            jax.ShapeDtypeStruct((LEAD, width), BF16),
            jax.ShapeDtypeStruct((rows, columns), BF16),
            jax.ShapeDtypeStruct((ROPE, rows), F32),
        ),
        cost_estimate=pl.CostEstimate(
            flops=2 * rows * width * 384, bytes_accessed=2_500_000, transcendentals=rows
        ),
        name="entry",
    )(tokens, gain.reshape(1, -1), latent_down, query_down.T, rotary_down.T)


LEAD = 16


def conv_kernel(
    mine_ref, other_ref, normed_ref, edge_ref, taps_ref, output_ref, out_ref,
    rows_ref, weight_ref, product_ref,
):
    core = lax.axis_index("core")
    near, _, _ = mine_ref.shape
    count, width = normed_ref.shape
    half = width // 2
    rows_ref[:LEAD, :] = edge_ref[...]
    rows_ref[LEAD:, :] = normed_ref[...]
    columns = weight_ref.shape[1]
    depth = 128 // near
    for side, ref in enumerate((mine_ref, other_ref)):
        for block in range(half // 128):
            for source in range(near):
                to = side * half + block * 128 + source * depth
                for b in range(columns // 128):
                    at = (block * (columns // 128) + b) * depth
                    weight_ref[to : to + depth, b * 128 : (b + 1) * 128] = ref[
                        source, at : at + depth, :
                    ]
    own = pl.ds(pl.multiple_of(core * half, half), half)
    rest = pl.ds(pl.multiple_of((1 - core) * half, half), half)
    spread = jnp.dot(rows_ref[:, own], weight_ref[:half, :], preferred_element_type=F32)
    spread += jnp.dot(rows_ref[:, rest], weight_ref[half:, :], preferred_element_type=F32)
    third = columns // 3
    product = spread[:, third : 2 * third] * spread[:, 2 * third :]
    product_ref[...] = product.astype(BF16).astype(F32)
    convolved = jnp.zeros((count, third), F32)
    for k in range(TAPS):
        first = LEAD - (TAPS - 1) + k
        convolved = convolved + product_ref[first : first + count, :] * taps_ref[k : k + 1, :]
    mixed = (spread[LEAD:, :third] * convolved).astype(BF16)
    for first in range(0, out_ref.shape[1], 512):
        at = slice(first, first + 512)
        out_ref[:, at] = jnp.dot(mixed, output_ref[:, at], preferred_element_type=F32)


def convolve(joint, joint_other, normed, edge, taps, output):
    count, width = normed.shape
    third, out_width = output.shape
    near = joint.shape[0]
    weights = pl.BlockSpec((near, joint.shape[1] - 2 * QUERY_ROWS, 128), lambda i: (0, 0, 0))
    whole = [pl.BlockSpec(a.shape, lambda i: (0, 0)) for a in (normed, edge, taps, output)]
    return pl.pallas_call(
        conv_kernel,
        out_shape=pltpu.HBM((count, out_width), F32),
        grid=(1,),
        in_specs=[weights, weights, *whole],
        out_specs=pl.BlockSpec((count, out_width), lambda i: (0, 0)),
        scratch_shapes=[
            pltpu.VMEM((LEAD + count, width), BF16),
            pltpu.VMEM((width, 3 * third), BF16),
            pltpu.VMEM((LEAD + count, third), F32),
        ],
        cost_estimate=pl.CostEstimate(
            flops=2 * count * (width * 3 * third + third * out_width),
            bytes_accessed=6_000_000,
            transcendentals=0,
        ),
        compiler_params=pltpu.CompilerParams(vmem_limit_bytes=30 << 20),
        name="convolve",
    )(
        joint,
        joint_other,
        pltpu.with_memory_space_constraint(normed, pltpu.HBM),
        edge,
        taps,
        pltpu.with_memory_space_constraint(output, pltpu.HBM),
    )


def merge_kernel(parts_ref, conv_ref, weight_ref, out_ref, top_ref, log_ref):
    groups = parts_ref.shape[0]
    tails = parts_ref[:, 128:PART_ROWS, :].astype(F32)
    heads = []
    for h in range(2):
        logs = tails[:, 8 * h, :] + (tails[:, 8 * h + 1, :] + tails[:, 8 * h + 2, :])
        top = jnp.max(logs, axis=0, keepdims=True)
        share = jnp.exp(logs - top)
        share_sum = jnp.sum(share, axis=0, keepdims=True)
        top_ref[h : h + 1, :] = top
        log_ref[h : h + 1, :] = jnp.log(share_sum)
        share = share / share_sum
        mixed = jnp.zeros((VDIM, 128), F32)
        for g in range(groups):
            part = parts_ref[g, h * VDIM : (h + 1) * VDIM, :].astype(F32)
            mixed = mixed + part * share[g : g + 1, :]
        heads.append(mixed)
    mixed = jnp.concatenate(heads, axis=0).T.astype(BF16)
    for first in range(0, out_ref.shape[1], 512):
        at = slice(first, first + 512)
        out_ref[:, at] = (
            conv_ref[:, at]
            + jnp.dot(mixed, weight_ref[:, at], preferred_element_type=F32)
        ).astype(BF16)


def merge(parts, conv_projected, heads_output):
    rows, width = conv_projected.shape
    return pl.pallas_call(
        merge_kernel,
        out_shape=(
            jax.ShapeDtypeStruct((rows, width), BF16),
            jax.ShapeDtypeStruct((2, rows), F32),
            jax.ShapeDtypeStruct((2, rows), F32),
        ),
        cost_estimate=pl.CostEstimate(
            flops=2 * rows * width * 128, bytes_accessed=2_000_000, transcendentals=rows * 32
        ),
        compiler_params=pltpu.CompilerParams(vmem_limit_bytes=16 << 20),
        name="merge",
    )(
        parts,
        pltpu.with_memory_space_constraint(conv_projected, pltpu.HBM),
        pltpu.with_memory_space_constraint(heads_output, pltpu.HBM),
    )


def layer(
    tokens,
    pre_gain,
    outer_gate,
    inner_gate,
    conv_input,
    conv_taps,
    query_down,
    latent_down,
    rotary_down,
    query_gain,
    latent_gain,
    query_up,
    query_rotary,
    key_up,
    value_up,
    conv_output,
    heads_output,
    post_gain,
):
    rows = tokens.shape[0]
    sp_index = lax.axis_index(SP)

    gates = spread_gates((outer_gate, inner_gate, conv_input), lax.axis_size(Z))
    gates = exchange(gates, Z)

    normed, tail, latents, key_raw = entry(tokens, pre_gain, latent_down, query_down, rotary_down)
    edge = shifted(tail, SP, 1)
    latents = lax.all_gather(latents, "tp", axis=0)

    positions = sp_index * rows + jnp.arange(rows, dtype=jnp.int32)
    frequency = rope_theta ** (-jnp.arange(ROPE // 2, dtype=F32) / (ROPE // 2))
    angles = positions.astype(F32)[None, :] * frequency[:, None]
    cosine, sine = jnp.cos(angles), jnp.sin(angles)
    key_turned = rotate_rows(key_raw, cosine, sine).astype(BF16)

    n_latent = latent_down.shape[1]
    key_latent = jnp.moveaxis(latents[:, :, :n_latent], 0, 1).reshape(rows, -1)
    query_latent = jnp.moveaxis(latents[:, :, n_latent:], 0, 1).reshape(rows, -1)
    latent_normed = rms_scale(key_latent, latent_gain).astype(BF16)
    query_normed = rms_scale(query_latent, query_gain).astype(BF16)
    query_nope = dot_t(query_normed, query_up).astype(BF16)
    turned = dot_t(query_normed, query_rotary).reshape(-1, ROPE, rows)
    turned = rotate_rows(turned, cosine, sine).astype(BF16).reshape(-1, rows)
    queries = jnp.concatenate([query_nope, turned], axis=0)
    queries_other = lax.ppermute(queries, "pair", [(0, 1), (1, 0)])
    first_of_pair = lax.axis_index("pair") == 0
    both = [
        jnp.where(first_of_pair, queries, queries_other),
        jnp.where(first_of_pair, queries_other, queries),
    ]
    _, wide, cores = (lax.axis_size(name) for name in GROUP)
    halves = gates.reshape(cores, -1, 128)
    both = jnp.broadcast_to(jnp.concatenate(both, axis=0), (wide, cores, 2 * QUERY_ROWS, 128))
    halves = jnp.broadcast_to(halves, (wide, *halves.shape))
    sent = jnp.concatenate([halves, both], axis=2)
    joint = exchange(sent.reshape(-1, *sent.shape[2:]), GROUP[1:])
    joint_other = lax.ppermute(joint, "core", [(0, 1), (1, 0)])
    held = jnp.concatenate(
        [
            dot_t(latent_normed, key_up).astype(BF16),
            key_turned,
            dot_t(latent_normed, value_up).astype(BF16),
        ],
        axis=0,
    )
    held = lax.all_gather(held, "far", axis=0, tiled=True).reshape(-1, *held.shape)

    parts = attend(held, joint)
    parts = exchange(parts, GROUP)

    conv_projected = convolve(
        joint,
        joint_other,
        normed,
        edge,
        conv_taps,
        conv_output,
    )
    projected, top, log_total = merge(parts, conv_projected, heads_output)
    tp = lax.axis_size("tp")
    arrived = exchange(projected.reshape(tp, rows // tp, -1), "tp")
    row_logsum = top + log_total
    projected = arrived.astype(F32).sum(axis=0)
    mixed = rms_scale(projected, post_gain).astype(BF16)
    return (mixed, row_logsum)


def solution(mesh):
    split = Mesh(mesh.devices.reshape(8, 2, 4, 2, mesh.shape["tp"]), SP_TP)
    return jax.shard_map(
        layer,
        mesh=split,
        in_specs=(
            P(SP, None),
            P(),
            P(SP, "tp"),
            P(SP, "tp"),
            P(SP, "tp"),
            P(None, "tp"),
            P(None, "tp"),
            P(None, "tp"),
            P(),
            P(),
            P(),
            P(None, "tp"),
            P(None, "tp"),
            P(None, "tp"),
            P(None, "tp"),
            P("tp", None),
            P("tp", None),
            P(),
        ),
        out_specs=(P(SP_TP, None), P("tp", SP)),
        check_vma=False,
    )
```

```python
import math

import jax
import jax.numpy as jnp
from jax import lax
from jax.experimental import pallas as pl
from jax.experimental.pallas import tpu as pltpu
from jax.sharding import Mesh
from jax.sharding import PartitionSpec as P

NOPE = 64
ROPE = 32
VDIM = 64
TAPS = 3
SP = ("far", "pair", "x", "core")
SP_TP = ("far", "pair", "x", "core", "tp")
Z = ("far", "pair")
GROUP = ("pair", "x", "core")

eps = 1e-06
rope_theta = 500000.0
SCALE = (NOPE + ROPE) ** (-0.5)
LOG2E = math.log2(math.e)
LOW = -1e30
BF16 = jnp.bfloat16
F32 = jnp.float32


def exchange(array, axis):
    return lax.all_to_all(array, axis, split_axis=0, concat_axis=0, tiled=True)


def shifted(value, axis, steps):
    count = lax.axis_size(axis)
    first, last = (max(0, -steps), min(count, count - steps))
    return lax.ppermute(value, axis, [(source, source + steps) for source in range(first, last)])


def rms_scale(values, scale_row):
    widened = values.astype(F32)
    return (
        widened * lax.rsqrt(jnp.mean(widened * widened, axis=-1, keepdims=True) + eps) * scale_row
    )


def dot_t(values, weights):
    return lax.dot_general(weights, values, (((0,), (1,)), ((), ())), preferred_element_type=F32)


def rotate_rows(values, cosine, sine):
    half = values.shape[-2] // 2
    leading = values[..., :half, :]
    trailing = values[..., half:, :]
    return jnp.concatenate(
        [leading * cosine - trailing * sine, trailing * cosine + leading * sine], axis=-2
    )


COLS = 256
QUERY_ROWS = 192
PART_ROWS = 144
FLOOR = -1e29


def attention_kernel(held_ref, query_ref, out_ref, key_rows, value_cols, query_full):
    far, here = lax.axis_index("far"), lax.axis_index(GROUP)
    blocks = held_ref.shape[0]
    near = query_ref.shape[0]
    groups = 2 * near
    queries = groups * 128
    pair = lax.axis_index("pair")
    for b in range(blocks):
        key_rows[b * 128 : (b + 1) * 128, :] = held_ref[b, 0:160, :].T
        value_cols[:, b * 128 : (b + 1) * 128] = held_ref[b, 160:288, :]
    for h in range(2):
        for g in range(groups):
            at = slice(h * queries + g * 128, h * queries + (g + 1) * 128)
            first = g // near * QUERY_ROWS
            query_full[h * 64 : (h + 1) * 64, at] = query_ref[
                g % near, first + h * 64 : first + (h + 1) * 64, :
            ]
            query_full[(1 - h) * 64 : (2 - h) * 64, at] = jnp.zeros((64, 128), BF16)
            query_full[128:160, at] = query_ref[
                g % near, first + 128 + h * 32 : first + 160 + h * 32, :
            ]
    factor = SCALE * LOG2E
    row = lax.broadcasted_iota(jnp.int32, (blocks * 128, 1), 0)
    key_at = row // 128 * queries + here * 128 + row % 128 - far * queries

    def score(first):
        return jnp.dot(
            key_rows[...], query_full[:, first : first + COLS], preferred_element_type=F32
        )

    def soften(first, scores):
        side = pair if first % queries < near * 128 else 1 - pair
        col = lax.broadcasted_iota(jnp.int32, (1, COLS), 1) + first % (near * 128)
        col = col + side * (near * 128)
        scores = jnp.where(key_at <= col, scores, LOW)
        best = jnp.maximum(jnp.max(scores, axis=0, keepdims=True), FLOOR)
        weights = jnp.exp2(scores * factor - best * factor)
        total = jnp.maximum(jnp.sum(weights, axis=0, keepdims=True), 1e-30)
        return weights.astype(BF16), total, best * SCALE + jnp.log(total)

    logs = {}

    def mix(first, weights, total, logsum):
        h = first // queries
        mixed = jnp.dot(
            value_cols[h * 64 : (h + 1) * 64, :], weights, preferred_element_type=F32
        )
        mixed = (mixed * (1.0 / total)).astype(BF16)
        high = logsum.astype(BF16).astype(F32)
        middle = (logsum - high).astype(BF16).astype(F32)
        low = logsum - high - middle
        tail = jnp.concatenate([high, middle, low, jnp.zeros((5, COLS), F32)], axis=0)
        for i in range(COLS // 128):
            g = first % queries // 128 + i
            side = pair if g < near else 1 - pair
            to = side * near + g % near
            at = slice(i * 128, (i + 1) * 128)
            out_ref[to, h * 64 : (h + 1) * 64, :] = mixed[:, at]
            if h == 0:
                logs[g] = tail[:, at]
            else:
                both = jnp.concatenate([logs.pop(g), tail[:, at]], axis=0)
                out_ref[to, 128:PART_ROWS, :] = both.astype(BF16)

    tiles = 2 * queries // COLS
    scores, softened = {}, {}
    for n in range(tiles + 2):
        if 0 <= n - 1 < tiles:
            softened[n - 1] = soften((n - 1) * COLS, scores.pop(n - 1))
        if n < tiles:
            scores[n] = score(n * COLS)
        if 0 <= n - 2 < tiles:
            mix((n - 2) * COLS, *softened.pop(n - 2))


def attend(held, joint):
    blocks, groups = held.shape[0], 2 * joint.shape[0]
    width = 2 * groups * 128
    return pl.pallas_call(
        attention_kernel,
        out_shape=pltpu.HBM((groups, PART_ROWS, 128), BF16),
        grid=(1,),
        in_specs=[
            pl.BlockSpec(held.shape, lambda i: (0, 0, 0)),
            pl.BlockSpec((groups // 2, 2 * QUERY_ROWS, 128), lambda i: (0, 2, 0)),
        ],
        out_specs=pl.BlockSpec((groups, PART_ROWS, 128), lambda i: (0, 0, 0)),
        scratch_shapes=[
            pltpu.VMEM((blocks * 128, 160), BF16),
            pltpu.VMEM((128, blocks * 128), BF16),
            pltpu.VMEM((160, width), BF16),
        ],
        compiler_params=pltpu.CompilerParams(vmem_limit_bytes=48 << 20),
        cost_estimate=pl.CostEstimate(
            flops=2 * blocks * 128 * width * (160 + 64),
            bytes_accessed=2_000_000,
            transcendentals=blocks * 128 * width,
        ),
        name="attend",
    )(held, joint)


def dot_nt(left, right):
    return lax.dot_general(left, right, (((1,), (1,)), ((), ())), preferred_element_type=F32)


def gates_kernel(outer_ref, inner_ref, signal_ref, out_ref):
    depth = outer_ref.shape[0]
    at = 0
    for ref in (outer_ref, inner_ref, signal_ref):
        for first in range(0, ref.shape[1], 128):
            block = ref[:, first : first + 128]
            for d in range(out_ref.shape[0]):
                out_ref[d, at : at + depth, :] = block
            at += depth


def spread_gates(gates, copies):
    depth, width = gates[0].shape
    return pl.pallas_call(
        gates_kernel,
        out_shape=jax.ShapeDtypeStruct((copies, 3 * depth * width // 128, 128), BF16),
        cost_estimate=pl.CostEstimate(flops=1_000_000, bytes_accessed=400_000, transcendentals=0),
        name="spread_gates",
    )(*gates)


def entry_kernel(
    tokens, gain, latent_down, query_down, rotary_down, normed_ref, tail_ref, latent_ref, rot_ref
):
    wide = tokens[...].astype(F32)
    scale = lax.rsqrt(jnp.mean(wide * wide, axis=-1, keepdims=True) + eps)
    normed = (wide * scale * gain[...]).astype(BF16)
    normed_ref[...] = normed
    tail_ref[...] = normed[normed.shape[0] - LEAD :, :]
    n = latent_down.shape[1]
    latent_ref[:, :n] = jnp.dot(
        normed, latent_down[...], preferred_element_type=F32
    ).astype(BF16)
    latent_ref[:, n:] = dot_nt(normed, query_down[...]).astype(BF16)
    rot_ref[...] = dot_nt(rotary_down[...], normed)


def entry(tokens, gain, latent_down, query_down, rotary_down):
    rows, width = tokens.shape
    columns = latent_down.shape[1] + query_down.shape[1]
    return pl.pallas_call(
        entry_kernel,
        out_shape=(
            jax.ShapeDtypeStruct((rows, width), BF16),
            jax.ShapeDtypeStruct((LEAD, width), BF16),
            jax.ShapeDtypeStruct((rows, columns), BF16),
            jax.ShapeDtypeStruct((ROPE, rows), F32),
        ),
        cost_estimate=pl.CostEstimate(
            flops=2 * rows * width * 384, bytes_accessed=2_500_000, transcendentals=rows
        ),
        name="entry",
    )(tokens, gain.reshape(1, -1), latent_down, query_down.T, rotary_down.T)


LEAD = 16


def conv_kernel(
    mine_ref, other_ref, normed_ref, edge_ref, taps_ref, output_ref, out_ref,
    rows_ref, weight_ref, product_ref,
):
    core = lax.axis_index("core")
    near, _, _ = mine_ref.shape
    count, width = normed_ref.shape
    half = width // 2
    rows_ref[:LEAD, :] = edge_ref[...]
    rows_ref[LEAD:, :] = normed_ref[...]
    columns = weight_ref.shape[1]
    depth = 128 // near
    for side, ref in enumerate((mine_ref, other_ref)):
        for block in range(half // 128):
            for source in range(near):
                to = side * half + block * 128 + source * depth
                for b in range(columns // 128):
                    at = (block * (columns // 128) + b) * depth
                    weight_ref[to : to + depth, b * 128 : (b + 1) * 128] = ref[
                        source, at : at + depth, :
                    ]
    own = pl.ds(pl.multiple_of(core * half, half), half)
    rest = pl.ds(pl.multiple_of((1 - core) * half, half), half)
    spread = jnp.dot(rows_ref[:, own], weight_ref[:half, :], preferred_element_type=F32)
    spread += jnp.dot(rows_ref[:, rest], weight_ref[half:, :], preferred_element_type=F32)
    third = columns // 3
    product = spread[:, third : 2 * third] * spread[:, 2 * third :]
    product_ref[...] = product.astype(BF16).astype(F32)
    convolved = jnp.zeros((count, third), F32)
    for k in range(TAPS):
        first = LEAD - (TAPS - 1) + k
        convolved = convolved + product_ref[first : first + count, :] * taps_ref[k : k + 1, :]
    mixed = (spread[LEAD:, :third] * convolved).astype(BF16)
    for first in range(0, out_ref.shape[1], 512):
        at = slice(first, first + 512)
        out_ref[:, at] = jnp.dot(mixed, output_ref[:, at], preferred_element_type=F32)


def convolve(joint, joint_other, normed, edge, taps, output):
    count, width = normed.shape
    third, out_width = output.shape
    near = joint.shape[0]
    weights = pl.BlockSpec((near, joint.shape[1] - 2 * QUERY_ROWS, 128), lambda i: (0, 0, 0))
    whole = [pl.BlockSpec(a.shape, lambda i: (0, 0)) for a in (normed, edge, taps, output)]
    return pl.pallas_call(
        conv_kernel,
        out_shape=pltpu.HBM((count, out_width), F32),
        grid=(1,),
        in_specs=[weights, weights, *whole],
        out_specs=pl.BlockSpec((count, out_width), lambda i: (0, 0)),
        scratch_shapes=[
            pltpu.VMEM((LEAD + count, width), BF16),
            pltpu.VMEM((width, 3 * third), BF16),
            pltpu.VMEM((LEAD + count, third), F32),
        ],
        cost_estimate=pl.CostEstimate(
            flops=2 * count * (width * 3 * third + third * out_width),
            bytes_accessed=6_000_000,
            transcendentals=0,
        ),
        compiler_params=pltpu.CompilerParams(vmem_limit_bytes=30 << 20),
        name="convolve",
    )(
        joint,
        joint_other,
        pltpu.with_memory_space_constraint(normed, pltpu.HBM),
        edge,
        taps,
        pltpu.with_memory_space_constraint(output, pltpu.HBM),
    )


def merge_kernel(parts_ref, conv_ref, weight_ref, out_ref, top_ref, log_ref, mixed_ref):
    @pl.when(pl.program_id(0) == 0)
    def mix():
        groups = parts_ref.shape[0]
        tails = parts_ref[:, 128:PART_ROWS, :].astype(F32)
        heads = []
        for h in range(2):
            logs = tails[:, 8 * h, :] + (tails[:, 8 * h + 1, :] + tails[:, 8 * h + 2, :])
            top = jnp.max(logs, axis=0, keepdims=True)
            share = jnp.exp(logs - top)
            share_sum = jnp.sum(share, axis=0, keepdims=True)
            top_ref[h : h + 1, :] = top
            log_ref[h : h + 1, :] = jnp.log(share_sum)
            share = share / share_sum
            mixed = jnp.zeros((VDIM, 128), F32)
            for g in range(groups):
                part = parts_ref[g, h * VDIM : (h + 1) * VDIM, :].astype(F32)
                mixed = mixed + part * share[g : g + 1, :]
            heads.append(mixed)
        mixed_ref[...] = jnp.concatenate(heads, axis=0).T.astype(BF16)

    added = jnp.dot(mixed_ref[...], weight_ref[...], preferred_element_type=F32)
    out_ref[...] = (conv_ref[...] + added).astype(BF16)


def merge(parts, conv_projected, heads_output):
    rows, width = conv_projected.shape
    step = width // 4
    columns = pl.BlockSpec((rows, step), lambda i: (0, i))
    small = pl.BlockSpec((2, rows), lambda i: (0, 0))
    return pl.pallas_call(
        merge_kernel,
        out_shape=(
            jax.ShapeDtypeStruct((rows, width), BF16),
            jax.ShapeDtypeStruct((2, rows), F32),
            jax.ShapeDtypeStruct((2, rows), F32),
        ),
        grid=(width // step,),
        in_specs=[
            pl.BlockSpec(parts.shape, lambda i: (0, 0, 0)),
            columns,
            pl.BlockSpec((heads_output.shape[0], step), lambda i: (0, i)),
        ],
        out_specs=(columns, small, small),
        scratch_shapes=[pltpu.VMEM((rows, heads_output.shape[0]), BF16)],
        cost_estimate=pl.CostEstimate(
            flops=2 * rows * width * 128, bytes_accessed=2_000_000, transcendentals=rows * 32
        ),
        compiler_params=pltpu.CompilerParams(vmem_limit_bytes=16 << 20),
        name="merge",
    )(
        parts,
        pltpu.with_memory_space_constraint(conv_projected, pltpu.HBM),
        pltpu.with_memory_space_constraint(heads_output, pltpu.HBM),
    )


def layer(
    tokens,
    pre_gain,
    outer_gate,
    inner_gate,
    conv_input,
    conv_taps,
    query_down,
    latent_down,
    rotary_down,
    query_gain,
    latent_gain,
    query_up,
    query_rotary,
    key_up,
    value_up,
    conv_output,
    heads_output,
    post_gain,
):
    rows = tokens.shape[0]
    sp_index = lax.axis_index(SP)

    gates = spread_gates((outer_gate, inner_gate, conv_input), lax.axis_size(Z))
    gates = exchange(gates, Z)

    normed, tail, latents, key_raw = entry(tokens, pre_gain, latent_down, query_down, rotary_down)
    edge = shifted(tail, SP, 1)
    latents = lax.all_gather(latents, "tp", axis=0)

    positions = sp_index * rows + jnp.arange(rows, dtype=jnp.int32)
    frequency = rope_theta ** (-jnp.arange(ROPE // 2, dtype=F32) / (ROPE // 2))
    angles = positions.astype(F32)[None, :] * frequency[:, None]
    cosine, sine = jnp.cos(angles), jnp.sin(angles)
    key_turned = rotate_rows(key_raw, cosine, sine).astype(BF16)

    n_latent = latent_down.shape[1]
    key_latent = jnp.moveaxis(latents[:, :, :n_latent], 0, 1).reshape(rows, -1)
    query_latent = jnp.moveaxis(latents[:, :, n_latent:], 0, 1).reshape(rows, -1)
    latent_normed = rms_scale(key_latent, latent_gain).astype(BF16)
    query_normed = rms_scale(query_latent, query_gain).astype(BF16)
    query_nope = dot_t(query_normed, query_up).astype(BF16)
    turned = dot_t(query_normed, query_rotary).reshape(-1, ROPE, rows)
    turned = rotate_rows(turned, cosine, sine).astype(BF16).reshape(-1, rows)
    queries = jnp.concatenate([query_nope, turned], axis=0)
    queries_other = lax.ppermute(queries, "pair", [(0, 1), (1, 0)])
    _, wide, cores = (lax.axis_size(name) for name in GROUP)
    halves = gates.reshape(cores, -1, 128)
    halves = jnp.broadcast_to(halves, (wide, *halves.shape))
    both = [jnp.broadcast_to(q, (wide, cores, *q.shape)) for q in (queries, queries_other)]
    sent = jnp.concatenate([halves, *both], axis=2)
    joint = exchange(sent.reshape(-1, *sent.shape[2:]), GROUP[1:])
    joint_other = lax.ppermute(joint, "core", [(0, 1), (1, 0)])
    held = jnp.concatenate(
        [
            dot_t(latent_normed, key_up).astype(BF16),
            key_turned,
            dot_t(latent_normed, value_up).astype(BF16),
        ],
        axis=0,
    )
    held = lax.all_gather(held, "far", axis=0, tiled=True).reshape(-1, *held.shape)

    parts = attend(held, joint)
    parts = exchange(parts, GROUP)

    conv_projected = convolve(
        joint,
        joint_other,
        normed,
        edge,
        conv_taps,
        conv_output,
    )
    projected, top, log_total = merge(parts, conv_projected, heads_output)
    tp = lax.axis_size("tp")
    arrived = exchange(projected.reshape(tp, rows // tp, -1), "tp")
    row_logsum = top + log_total
    projected = arrived.astype(F32).sum(axis=0)
    mixed = rms_scale(projected, post_gain).astype(BF16)
    return (mixed, row_logsum)


def solution(mesh):
    split = Mesh(mesh.devices.reshape(8, 2, 4, 2, mesh.shape["tp"]), SP_TP)
    return jax.shard_map(
        layer,
        mesh=split,
        in_specs=(
            P(SP, None),
            P(),
            P(SP, "tp"),
            P(SP, "tp"),
            P(SP, "tp"),
            P(None, "tp"),
            P(None, "tp"),
            P(None, "tp"),
            P(),
            P(),
            P(),
            P(None, "tp"),
            P(None, "tp"),
            P(None, "tp"),
            P(None, "tp"),
            P("tp", None),
            P("tp", None),
            P(),
        ),
        out_specs=(P(SP_TP, None), P("tp", SP)),
        check_vma=False,
    )
```

```python
import math

import jax
import jax.numpy as jnp
from jax import lax
from jax.experimental import pallas as pl
from jax.experimental.pallas import tpu as pltpu
from jax.sharding import Mesh
from jax.sharding import PartitionSpec as P

NOPE = 64
ROPE = 32
VDIM = 64
TAPS = 3
SP = ("far", "pair", "x", "core")
SP_TP = ("far", "pair", "x", "core", "tp")
Z = ("far", "pair")
GROUP = ("pair", "x", "core")

eps = 1e-06
rope_theta = 500000.0
SCALE = (NOPE + ROPE) ** (-0.5)
LOG2E = math.log2(math.e)
LOW = -1e30
BF16 = jnp.bfloat16
F32 = jnp.float32


def exchange(array, axis):
    return lax.all_to_all(array, axis, split_axis=0, concat_axis=0, tiled=True)


def shifted(value, axis, steps):
    count = lax.axis_size(axis)
    first, last = (max(0, -steps), min(count, count - steps))
    return lax.ppermute(value, axis, [(source, source + steps) for source in range(first, last)])


def rms_scale(values, scale_row):
    widened = values.astype(F32)
    return (
        widened * lax.rsqrt(jnp.mean(widened * widened, axis=-1, keepdims=True) + eps) * scale_row
    )


def dot_t(values, weights):
    return lax.dot_general(weights, values, (((0,), (1,)), ((), ())), preferred_element_type=F32)


def rotate_rows(values, cosine, sine):
    half = values.shape[-2] // 2
    leading = values[..., :half, :]
    trailing = values[..., half:, :]
    return jnp.concatenate(
        [leading * cosine - trailing * sine, trailing * cosine + leading * sine], axis=-2
    )


COLS = 256
QUERY_ROWS = 192
PART_ROWS = 144
FLOOR = -1e29


def attention_kernel(held_ref, query_ref, out_ref, key_rows, value_cols, query_full):
    far, here = lax.axis_index("far"), lax.axis_index(GROUP)
    blocks = held_ref.shape[0]
    near = query_ref.shape[0]
    groups = 2 * near
    queries = groups * 128
    pair = lax.axis_index("pair")
    for b in range(blocks):
        key_rows[b * 128 : (b + 1) * 128, :] = held_ref[b, 0:160, :].T
        value_cols[:, b * 128 : (b + 1) * 128] = held_ref[b, 160:288, :]
    for h in range(2):
        for g in range(groups):
            at = slice(h * queries + g * 128, h * queries + (g + 1) * 128)
            first = g // near * QUERY_ROWS
            query_full[h * 64 : (h + 1) * 64, at] = query_ref[
                g % near, first + h * 64 : first + (h + 1) * 64, :
            ]
            query_full[(1 - h) * 64 : (2 - h) * 64, at] = jnp.zeros((64, 128), BF16)
            query_full[128:160, at] = query_ref[
                g % near, first + 128 + h * 32 : first + 160 + h * 32, :
            ]
    factor = SCALE * LOG2E
    row = lax.broadcasted_iota(jnp.int32, (blocks * 128, 1), 0)
    key_at = row // 128 * queries + here * 128 + row % 128 - far * queries

    def score(first):
        return jnp.dot(
            key_rows[...], query_full[:, first : first + COLS], preferred_element_type=F32
        )

    def soften(first, scores):
        side = pair if first % queries < near * 128 else 1 - pair
        col = lax.broadcasted_iota(jnp.int32, (1, COLS), 1) + first % (near * 128)
        col = col + side * (near * 128)
        scores = jnp.where(key_at <= col, scores, LOW)
        best = jnp.maximum(jnp.max(scores, axis=0, keepdims=True), FLOOR)
        weights = jnp.exp2(scores * factor - best * factor)
        total = jnp.maximum(jnp.sum(weights, axis=0, keepdims=True), 1e-30)
        return weights.astype(BF16), total, best * SCALE + jnp.log(total)

    logs = {}

    def mix(first, weights, total, logsum):
        h = first // queries
        mixed = jnp.dot(
            value_cols[h * 64 : (h + 1) * 64, :], weights, preferred_element_type=F32
        )
        mixed = (mixed * (1.0 / total)).astype(BF16)
        high = logsum.astype(BF16).astype(F32)
        middle = (logsum - high).astype(BF16).astype(F32)
        low = logsum - high - middle
        tail = jnp.concatenate([high, middle, low, jnp.zeros((5, COLS), F32)], axis=0)
        for i in range(COLS // 128):
            g = first % queries // 128 + i
            side = pair if g < near else 1 - pair
            to = side * near + g % near
            at = slice(i * 128, (i + 1) * 128)
            out_ref[to, h * 64 : (h + 1) * 64, :] = mixed[:, at]
            if h == 0:
                logs[g] = tail[:, at]
            else:
                both = jnp.concatenate([logs.pop(g), tail[:, at]], axis=0)
                out_ref[to, 128:PART_ROWS, :] = both.astype(BF16)

    tiles = 2 * queries // COLS
    scores, softened = {}, {}
    for n in range(tiles + 2):
        if 0 <= n - 1 < tiles:
            softened[n - 1] = soften((n - 1) * COLS, scores.pop(n - 1))
        if n < tiles:
            scores[n] = score(n * COLS)
        if 0 <= n - 2 < tiles:
            mix((n - 2) * COLS, *softened.pop(n - 2))


def attend(held, joint):
    blocks, groups = held.shape[0], 2 * joint.shape[0]
    width = 2 * groups * 128
    return pl.pallas_call(
        attention_kernel,
        out_shape=pltpu.HBM((groups, PART_ROWS, 128), BF16),
        grid=(1,),
        in_specs=[
            pl.BlockSpec(held.shape, lambda i: (0, 0, 0)),
            pl.BlockSpec((groups // 2, 2 * QUERY_ROWS, 128), lambda i: (0, 2, 0)),
        ],
        out_specs=pl.BlockSpec((groups, PART_ROWS, 128), lambda i: (0, 0, 0)),
        scratch_shapes=[
            pltpu.VMEM((blocks * 128, 160), BF16),
            pltpu.VMEM((128, blocks * 128), BF16),
            pltpu.VMEM((160, width), BF16),
        ],
        compiler_params=pltpu.CompilerParams(vmem_limit_bytes=48 << 20),
        cost_estimate=pl.CostEstimate(
            flops=2 * blocks * 128 * width * (160 + 64),
            bytes_accessed=2_000_000,
            transcendentals=blocks * 128 * width,
        ),
        name="attend",
    )(held, joint)


def dot_nt(left, right):
    return lax.dot_general(left, right, (((1,), (1,)), ((), ())), preferred_element_type=F32)


def gates_kernel(outer_ref, inner_ref, signal_ref, out_ref):
    depth = outer_ref.shape[0]
    at = 0
    for ref in (outer_ref, inner_ref, signal_ref):
        for first in range(0, ref.shape[1], 128):
            block = ref[:, first : first + 128]
            for d in range(out_ref.shape[0]):
                out_ref[d, at : at + depth, :] = block
            at += depth


def spread_gates(gates, copies):
    depth, width = gates[0].shape
    return pl.pallas_call(
        gates_kernel,
        out_shape=jax.ShapeDtypeStruct((copies, 3 * depth * width // 128, 128), BF16),
        cost_estimate=pl.CostEstimate(flops=1_000_000, bytes_accessed=400_000, transcendentals=0),
        name="spread_gates",
    )(*gates)


def entry_kernel(
    tokens, gain, latent_down, query_down, rotary_down, normed_ref, tail_ref, latent_ref, rot_ref
):
    wide = tokens[...].astype(F32)
    scale = lax.rsqrt(jnp.mean(wide * wide, axis=-1, keepdims=True) + eps)
    normed = (wide * scale * gain[...]).astype(BF16)
    normed_ref[...] = normed
    tail_ref[...] = normed[normed.shape[0] - LEAD :, :]
    n = latent_down.shape[1]
    latent_ref[:, :n] = jnp.dot(
        normed, latent_down[...], preferred_element_type=F32
    ).astype(BF16)
    latent_ref[:, n:] = dot_nt(normed, query_down[...]).astype(BF16)
    rot_ref[...] = dot_nt(rotary_down[...], normed)


def entry(tokens, gain, latent_down, query_down, rotary_down):
    rows, width = tokens.shape
    columns = latent_down.shape[1] + query_down.shape[1]
    return pl.pallas_call(
        entry_kernel,
        out_shape=(
            jax.ShapeDtypeStruct((rows, width), BF16),
            jax.ShapeDtypeStruct((LEAD, width), BF16),
            jax.ShapeDtypeStruct((rows, columns), BF16),
            jax.ShapeDtypeStruct((ROPE, rows), F32),
        ),
        cost_estimate=pl.CostEstimate(
            flops=2 * rows * width * 384, bytes_accessed=2_500_000, transcendentals=rows
        ),
        name="entry",
    )(tokens, gain.reshape(1, -1), latent_down, query_down.T, rotary_down.T)


LEAD = 16
MERGE_STEPS = 1


def conv_kernel(
    mine_ref, other_ref, normed_ref, edge_ref, taps_ref, out_ref,
    rows_ref, weight_ref, product_ref,
):
    core = lax.axis_index("core")
    near, _, _ = mine_ref.shape
    count, width = normed_ref.shape
    half = width // 2
    rows_ref[:LEAD, :] = edge_ref[...]
    rows_ref[LEAD:, :] = normed_ref[...]
    columns = weight_ref.shape[1]
    depth = 128 // near
    for side, ref in enumerate((mine_ref, other_ref)):
        for block in range(half // 128):
            for source in range(near):
                to = side * half + block * 128 + source * depth
                for b in range(columns // 128):
                    at = (block * (columns // 128) + b) * depth
                    weight_ref[to : to + depth, b * 128 : (b + 1) * 128] = ref[
                        source, at : at + depth, :
                    ]
    own = pl.ds(pl.multiple_of(core * half, half), half)
    rest = pl.ds(pl.multiple_of((1 - core) * half, half), half)
    spread = jnp.dot(rows_ref[:, own], weight_ref[:half, :], preferred_element_type=F32)
    spread += jnp.dot(rows_ref[:, rest], weight_ref[half:, :], preferred_element_type=F32)
    third = columns // 3
    product = spread[:, third : 2 * third] * spread[:, 2 * third :]
    product_ref[...] = product.astype(BF16).astype(F32)
    convolved = jnp.zeros((count, third), F32)
    for k in range(TAPS):
        first = LEAD - (TAPS - 1) + k
        convolved = convolved + product_ref[first : first + count, :] * taps_ref[k : k + 1, :]
    out_ref[...] = (spread[LEAD:, :third] * convolved).astype(BF16)


def convolve(joint, joint_other, normed, edge, taps):
    count, width = normed.shape
    third = taps.shape[1]
    near = joint.shape[0]
    weights = pl.BlockSpec((near, joint.shape[1] - 2 * QUERY_ROWS, 128), lambda i: (0, 0, 0))
    whole = [pl.BlockSpec(a.shape, lambda i: (0, 0)) for a in (normed, edge, taps)]
    return pl.pallas_call(
        conv_kernel,
        out_shape=jax.ShapeDtypeStruct((count, third), BF16),
        grid=(1,),
        in_specs=[weights, weights, *whole],
        out_specs=pl.BlockSpec((count, third), lambda i: (0, 0)),
        scratch_shapes=[
            pltpu.VMEM((LEAD + count, width), BF16),
            pltpu.VMEM((width, 3 * third), BF16),
            pltpu.VMEM((LEAD + count, third), F32),
        ],
        cost_estimate=pl.CostEstimate(
            flops=2 * count * width * 3 * third, bytes_accessed=4_000_000, transcendentals=0
        ),
        compiler_params=pltpu.CompilerParams(vmem_limit_bytes=30 << 20),
        name="convolve",
    )(joint, joint_other, pltpu.with_memory_space_constraint(normed, pltpu.HBM), edge, taps)


def merge_kernel(
    parts_ref, conv_ref, output_hbm, weight_hbm, out_ref, top_ref, log_ref,
    output_ref, weight_ref, output_sems, weight_sems,
):
    groups = parts_ref.shape[0]
    copies = []
    for i in range(MERGE_STEPS):
        width = out_ref.shape[1] // MERGE_STEPS
        at = slice(i * width, (i + 1) * width)
        pair = (
            pltpu.make_async_copy(output_hbm.at[:, at], output_ref.at[:, at], output_sems.at[i]),
            pltpu.make_async_copy(weight_hbm.at[:, at], weight_ref.at[:, at], weight_sems.at[i]),
        )
        for copy in pair:
            copy.start()
        copies.append((at, pair))
    tails = parts_ref[:, 128:PART_ROWS, :].astype(F32)
    heads = []
    for h in range(2):
        logs = tails[:, 8 * h, :] + (tails[:, 8 * h + 1, :] + tails[:, 8 * h + 2, :])
        top = jnp.max(logs, axis=0, keepdims=True)
        share = jnp.exp(logs - top)
        share_sum = jnp.sum(share, axis=0, keepdims=True)
        top_ref[h : h + 1, :] = top
        log_ref[h : h + 1, :] = jnp.log(share_sum)
        share = share / share_sum
        mixed = jnp.zeros((VDIM, 128), F32)
        for g in range(groups):
            part = parts_ref[g, h * VDIM : (h + 1) * VDIM, :].astype(F32)
            mixed = mixed + part * share[g : g + 1, :]
        heads.append(mixed)
    mixed = jnp.concatenate(heads, axis=0).T.astype(BF16)
    for at, pair in copies:
        for copy in pair:
            copy.wait()
        added = jnp.dot(conv_ref[...], output_ref[:, at], preferred_element_type=F32)
        added += jnp.dot(mixed, weight_ref[:, at], preferred_element_type=F32)
        out_ref[:, at] = added.astype(BF16)


def merge(parts, conv_mixed, conv_output, heads_output):
    rows, width = conv_mixed.shape[0], heads_output.shape[1]
    return pl.pallas_call(
        merge_kernel,
        out_shape=(
            jax.ShapeDtypeStruct((rows, width), BF16),
            jax.ShapeDtypeStruct((2, rows), F32),
            jax.ShapeDtypeStruct((2, rows), F32),
        ),
        in_specs=[
            pl.BlockSpec(memory_space=pltpu.VMEM),
            pl.BlockSpec(memory_space=pltpu.VMEM),
            pl.BlockSpec(memory_space=pltpu.HBM),
            pl.BlockSpec(memory_space=pltpu.HBM),
        ],
        scratch_shapes=[
            pltpu.VMEM(conv_output.shape, BF16),
            pltpu.VMEM(heads_output.shape, BF16),
            pltpu.SemaphoreType.DMA((MERGE_STEPS,)),
            pltpu.SemaphoreType.DMA((MERGE_STEPS,)),
        ],
        cost_estimate=pl.CostEstimate(
            flops=2 * rows * width * 384, bytes_accessed=2_500_000, transcendentals=rows * 32
        ),
        compiler_params=pltpu.CompilerParams(vmem_limit_bytes=16 << 20),
        name="merge",
    )(
        parts,
        conv_mixed,
        pltpu.with_memory_space_constraint(conv_output, pltpu.HBM),
        pltpu.with_memory_space_constraint(heads_output, pltpu.HBM),
    )


def layer(
    tokens,
    pre_gain,
    outer_gate,
    inner_gate,
    conv_input,
    conv_taps,
    query_down,
    latent_down,
    rotary_down,
    query_gain,
    latent_gain,
    query_up,
    query_rotary,
    key_up,
    value_up,
    conv_output,
    heads_output,
    post_gain,
):
    rows = tokens.shape[0]
    sp_index = lax.axis_index(SP)

    gates = spread_gates((outer_gate, inner_gate, conv_input), lax.axis_size(Z))
    gates = exchange(gates, Z)

    normed, tail, latents, key_raw = entry(tokens, pre_gain, latent_down, query_down, rotary_down)
    edge = shifted(tail, SP, 1)
    latents = lax.all_gather(latents, "tp", axis=0)

    positions = sp_index * rows + jnp.arange(rows, dtype=jnp.int32)
    frequency = rope_theta ** (-jnp.arange(ROPE // 2, dtype=F32) / (ROPE // 2))
    angles = positions.astype(F32)[None, :] * frequency[:, None]
    cosine, sine = jnp.cos(angles), jnp.sin(angles)
    key_turned = rotate_rows(key_raw, cosine, sine).astype(BF16)

    n_latent = latent_down.shape[1]
    key_latent = jnp.moveaxis(latents[:, :, :n_latent], 0, 1).reshape(rows, -1)
    query_latent = jnp.moveaxis(latents[:, :, n_latent:], 0, 1).reshape(rows, -1)
    latent_normed = rms_scale(key_latent, latent_gain).astype(BF16)
    query_normed = rms_scale(query_latent, query_gain).astype(BF16)
    query_nope = dot_t(query_normed, query_up).astype(BF16)
    turned = dot_t(query_normed, query_rotary).reshape(-1, ROPE, rows)
    turned = rotate_rows(turned, cosine, sine).astype(BF16).reshape(-1, rows)
    queries = jnp.concatenate([query_nope, turned], axis=0)
    queries_other = lax.ppermute(queries, "pair", [(0, 1), (1, 0)])
    _, wide, cores = (lax.axis_size(name) for name in GROUP)
    halves = gates.reshape(cores, -1, 128)
    halves = jnp.broadcast_to(halves, (wide, *halves.shape))
    both = [jnp.broadcast_to(q, (wide, cores, *q.shape)) for q in (queries, queries_other)]
    sent = jnp.concatenate([halves, *both], axis=2)
    joint = exchange(sent.reshape(-1, *sent.shape[2:]), GROUP[1:])
    joint_other = lax.ppermute(joint, "core", [(0, 1), (1, 0)])
    held = jnp.concatenate(
        [
            dot_t(latent_normed, key_up).astype(BF16),
            key_turned,
            dot_t(latent_normed, value_up).astype(BF16),
        ],
        axis=0,
    )
    held = lax.all_gather(held, "far", axis=0, tiled=True).reshape(-1, *held.shape)

    parts = attend(held, joint)
    parts = exchange(parts, GROUP)

    conv_mixed = convolve(joint, joint_other, normed, edge, conv_taps)

    projected, top, log_total = merge(parts, conv_mixed, conv_output, heads_output)
    tp = lax.axis_size("tp")
    arrived = exchange(projected.reshape(tp, rows // tp, -1), "tp")
    row_logsum = top + log_total
    projected = arrived.astype(F32).sum(axis=0)
    mixed = rms_scale(projected, post_gain).astype(BF16)
    return (mixed, row_logsum)


def solution(mesh):
    split = Mesh(mesh.devices.reshape(8, 2, 4, 2, mesh.shape["tp"]), SP_TP)
    return jax.shard_map(
        layer,
        mesh=split,
        in_specs=(
            P(SP, None),
            P(),
            P(SP, "tp"),
            P(SP, "tp"),
            P(SP, "tp"),
            P(None, "tp"),
            P(None, "tp"),
            P(None, "tp"),
            P(),
            P(),
            P(),
            P(None, "tp"),
            P(None, "tp"),
            P(None, "tp"),
            P(None, "tp"),
            P("tp", None),
            P("tp", None),
            P(),
        ),
        out_specs=(P(SP_TP, None), P("tp", SP)),
        check_vma=False,
    )
```
